256 devices in a mesh: grp: 2 (over y), sp: 16 (over z), tp: 8 (over x, core).
Axes of the slice: x: 4, y: 2, z: 16, core: 2. Of those that a mesh axis runs over, the one named last changes fastest.
The devices are a block of a 4x16x16 slice.
Arguments:
- queries: bfloat16 [24576, 1024], P(('grp', 'sp'), 'tp'), parts along dimension 0, may hold values from -8 to 8
- keys: bfloat16 [24576, 256], P(('grp', 'sp')), parts along dimension 0, may hold values from -8 to 8
- values: bfloat16 [24576, 256], P(('grp', 'sp')), parts along dimension 0, may hold values from -6 to 6
- query_gain: float32 [128], replicated, may hold values from 0.2 to 6
- key_gain: float32 [128], replicated, may hold values from 0.2 to 6
- residual: bfloat16 [24576, 2048], P(('grp', 'sp', 'tp')), parts along dimension 0, may hold values from -6 to 6
- out_weight: bfloat16 [1024, 2048], P('tp'), may hold values from -0.1875 to 0.1875
- mix_gain: float32 [2048], replicated, may hold values from 0.1 to 1.9
- ffn_gain: float32 [2048], replicated, may hold values from 0.1 to 1.9
- gate_in: bfloat16 [2048, 5632], P('sp', 'tp'), may hold values from -0.125 to 0.125
- value_in: bfloat16 [2048, 5632], P('sp', 'tp'), may hold values from -0.125 to 0.125
- conv_gate: float32 [3, 5632], P(None, 'tp'), may hold values from -3 to 3
- conv_value: float32 [3, 5632], P(None, 'tp'), may hold values from -3 to 3
- down_t: bfloat16 [2048, 5632], P('sp', 'tp'), may hold values from -0.078125 to 0.078125
Outputs:
- layer_out: bfloat16 [24576, 2048], P(('grp', 'sp', 'tp')), parts along dimension 0
The draws below stay inside these ranges and needn't reach their ends.
There are 2 independent parts, one for each index of `grp`. The reference program is written for one: setup_inputs(seed, part) draws one part's arguments, and reference() takes and returns one part's arrays. A program takes and returns all parts, laid end to end along the dimension named above; an argument that names none is the same for every part. Nothing has to cross between parts.
All inputs are finite; a program needn't handle non-finite values.
Results may differ from the reference program's by a relative error of at most 0.02.
The reference program's roundings to bfloat16 on the way count: a program that leaves them out, or rounds other values in their place, can miss the bound.
Values may be sent and summed in bfloat16 or wider, within the bound.
A program may use at most 128 MiB of HBM per device.

```python
import math
import jax
import jax.numpy as jnp
from jax import lax

D = 2048
HEADS = 8
KVH = 2
HD = 128
FF = 5632
GRID_W = 64
SEQ = 12288
N_TP = 8


def shared_keys(key):
    base = jax.random.normal(jax.random.fold_in(key, 11), (SEQ, KVH * HD), jnp.float32)
    return jnp.clip(base, -8.0, 8.0)


def draw_keys(key, part):
    base = shared_keys(key)
    return base.astype(jnp.bfloat16)


def draw_queries(key, part):
    drawn = jax.random.normal(jax.random.fold_in(key, 13), (SEQ, HEADS * HD), jnp.float32)
    return jnp.clip(drawn, -8.0, 8.0).astype(jnp.bfloat16)


def gain_draw(key):
    return jnp.clip(1.0 + 0.18 * jax.random.normal(key, (HD,), jnp.float32), 0.2, 2.0)


def draw_query_gain(key, part):
    return gain_draw(jax.random.fold_in(key, 21))


def draw_key_gain(key, part):
    return gain_draw(jax.random.fold_in(key, 22))


def shard_levels(own_key, extent, shards, low, top_value):
    factor_of, own = 1.0, jax.random.fold_in(own_key, 6)
    for position, blocks in shards:
        heights = jnp.exp(jax.random.uniform(jax.random.fold_in(own, position), (blocks,), jnp.float32, low / len(shards), top_value / len(shards)))
        factor_of = factor_of * jnp.repeat(heights, extent[position] // blocks).reshape([-1 if axis == position else 1 for axis in range(len(extent))])
    return factor_of


def centred(key, shape, scale, limit, cuts=(), held_as=jnp.bfloat16):
    result = jax.random.normal(key, shape, jnp.float32) * scale
    if len(cuts) > 0:
        result = shard_levels(key, shape, cuts, -0.22, 0.18) * result
    return jnp.clip(result, min=-limit, max=limit).astype(held_as)


def setup_inputs(seed: int = 0, part: int = 0) -> dict:
    arg_keys = jax.random.split(jax.random.key(seed), 15)
    own_keys = jax.random.split(jax.random.fold_in(arg_keys[14], part), 15)
    queries = draw_queries(jax.random.fold_in(jax.random.fold_in(arg_keys[14], part), 71), part)
    keys = draw_keys(jax.random.fold_in(jax.random.fold_in(arg_keys[14], part), 71), part)
    values = centred(own_keys[2], (SEQ, KVH * HD), 1.0, 6.0, ((0, 16),))
    query_gain = draw_query_gain(jax.random.fold_in(arg_keys[14], 71), part)
    key_gain = draw_key_gain(jax.random.fold_in(arg_keys[14], 71), part)
    residual = centred(own_keys[5], (SEQ, D), 1.0, 6.0, ((0, 128),))
    out_weight = centred(arg_keys[6], (HEADS * HD, D), (HEADS * HD) ** -0.5, 0.1875, ((0, 8),))
    mix_gain = jnp.clip(1.0 + 0.18 * jax.random.normal(arg_keys[7], (D,), jnp.float32), 0.1, 1.9)
    ffn_gain = jnp.clip(1.0 + 0.18 * jax.random.normal(arg_keys[8], (D,), jnp.float32), 0.1, 1.9)
    gate_in = centred(arg_keys[9], (D, FF), D ** -0.5, 0.125, ((0, 16), (1, 8)))
    value_in = centred(arg_keys[10], (D, FF), D ** -0.5, 0.125, ((0, 16), (1, 8)))
    conv_gate = centred(arg_keys[11], (3, FF), 0.577, 3.0, ((1, 8),), jnp.float32)
    conv_value = centred(arg_keys[12], (3, FF), 0.577, 3.0, ((1, 8),), jnp.float32)
    down_t = centred(arg_keys[13], (D, FF), FF ** -0.5, 0.078125, ((0, 16), (1, 8)))
    return dict(queries=queries, keys=keys, values=values, query_gain=query_gain, key_gain=key_gain, residual=residual, out_weight=out_weight, mix_gain=mix_gain, ffn_gain=ffn_gain, gate_in=gate_in, value_in=value_in, conv_gate=conv_gate, conv_value=conv_value, down_t=down_t)


EPSILON = 1e-06
THETA = 10000.0

def rotary_tables():
    quarter = HD // 4
    inverse = THETA ** (-(2.0 * jnp.arange(quarter, dtype=jnp.float32)) / (HD // 2))
    positions = jnp.arange(SEQ, dtype=jnp.int32)
    grid_row = (positions // GRID_W - SEQ // GRID_W // 2).astype(jnp.float32)
    grid_col = (positions % GRID_W - GRID_W // 2).astype(jnp.float32)
    row_angle = grid_row[:, None] * inverse[None, :]
    col_angle = grid_col[:, None] * inverse[None, :]
    angle = jnp.concatenate([row_angle, row_angle, col_angle, col_angle], axis=-1)
    return (jnp.cos(angle), jnp.sin(angle))

def rotate_quarters(vector):
    first, second, third, fourth = jnp.split(vector, 4, axis=-1)
    return jnp.concatenate([-second, first, -fourth, third], axis=-1)

def prepare_heads(raw, gain, cos_table, sin_table, factor):
    floats = raw.astype(jnp.float32)
    normed = floats * lax.rsqrt(lax.optimization_barrier(jnp.mean(floats * floats, axis=-1, keepdims=True)) + EPSILON) * gain
    turned = normed * cos_table + rotate_quarters(normed) * sin_table
    return (turned * factor).astype(jnp.bfloat16)

def rms_rows(stream, gain):
    floats = stream.astype(jnp.float32)
    return floats * lax.rsqrt(lax.optimization_barrier(jnp.mean(floats * floats, axis=-1, keepdims=True)) + EPSILON) * gain

def reference(queries, keys, values, query_gain, key_gain, residual, out_weight, mix_gain, ffn_gain, gate_in, value_in, conv_gate, conv_value, down_t):
    group = HEADS // KVH
    cos_table, sin_table = rotary_tables()
    query_rot = prepare_heads(queries.reshape(SEQ, HEADS, HD), query_gain, cos_table[:, None, :], sin_table[:, None, :], HD ** (-0.5))
    key_rot = prepare_heads(keys.reshape(SEQ, KVH, HD), key_gain, cos_table[:, None, :], sin_table[:, None, :], 1.0)
    key_float = key_rot.astype(jnp.float32)
    value_float = values.reshape(SEQ, KVH, HD).astype(jnp.float32)
    block = math.gcd(SEQ, 512)
    query_blocks = query_rot.reshape(SEQ // block, block, KVH, group, HD)

    def attend_block(query_block):
        scores = jnp.einsum('qhgd,khd->hgqk', query_block.astype(jnp.float32), key_float)
        highest = lax.optimization_barrier(jnp.max(scores, axis=-1, keepdims=True))
        weights = jnp.exp(scores - highest)
        denom = lax.optimization_barrier(jnp.sum(weights, axis=-1, keepdims=True))
        rounded = weights.astype(jnp.bfloat16).astype(jnp.float32)
        summed = jnp.einsum('hgqk,khd->qhgd', rounded, value_float)
        denom_t = jnp.transpose(denom, (2, 0, 1, 3))
        return (summed / denom_t).astype(jnp.bfloat16)
    attended = lax.map(attend_block, query_blocks).reshape(SEQ, HEADS * HD)
    head_cols = HEADS * HD // N_TP
    mix = jnp.zeros((SEQ, D), jnp.float32)
    for group_index in range(N_TP):
        lower = group_index * head_cols
        partial_mix = jnp.dot(attended[:, lower:lower + head_cols], out_weight[lower:lower + head_cols], preferred_element_type=jnp.float32).astype(jnp.bfloat16)
        partial_mix = lax.optimization_barrier(partial_mix)
        mix = mix + partial_mix.astype(jnp.float32)
    mix_normed = rms_rows(mix, mix_gain)
    stream = (residual.astype(jnp.float32) + mix_normed).astype(jnp.bfloat16)
    normed = rms_rows(stream, ffn_gain).astype(jnp.bfloat16)
    gate_up = jnp.dot(normed, gate_in, preferred_element_type=jnp.float32).astype(jnp.bfloat16)
    value_up = jnp.dot(normed, value_in, preferred_element_type=jnp.float32).astype(jnp.bfloat16)

    def depthwise(upward, taps):
        padded = jnp.pad(upward.astype(jnp.float32), ((1, 1), (0, 0)))
        return taps[0] * padded[:-2] + taps[1] * padded[1:-1] + taps[2] * padded[2:]
    gate_mixed = depthwise(gate_up, conv_gate)
    value_mixed = depthwise(value_up, conv_value)
    hidden = (jax.nn.gelu(gate_mixed, approximate=True) * value_mixed).astype(jnp.bfloat16)
    unit_cols = FF // N_TP
    ffn_out = jnp.zeros((SEQ, D), jnp.float32)
    for group_index in range(N_TP):
        lower = group_index * unit_cols
        partial_down = jnp.dot(hidden[:, lower:lower + unit_cols], down_t[:, lower:lower + unit_cols].T, preferred_element_type=jnp.float32).astype(jnp.bfloat16)
        partial_down = lax.optimization_barrier(partial_down)
        ffn_out = ffn_out + partial_down.astype(jnp.float32)
    return (stream.astype(jnp.float32) + ffn_out).astype(jnp.bfloat16)
```

```python
import functools

import jax
import jax.numpy as jnp
import numpy as np
from jax import lax
from jax.experimental import pallas as pl
from jax.experimental.pallas import tpu as pltpu
from jax.sharding import PartitionSpec as P

HEADS = 8
KVH = 2
GRID_W = 64
EPSILON = 1e-06
THETA = 10000.0
LANES = 128
MESH = pl.DeviceIdType.MESH
F32 = jnp.float32
BF16 = jnp.bfloat16


def rotary_tables(seq_total, head_dim):
    quarter = head_dim // 4
    inverse = np.float32(THETA) ** (
        -(np.float32(2.0) * np.arange(quarter, dtype=np.float32)) / np.float32(head_dim // 2)
    )
    inverse = inverse.astype(np.float32)
    rows = (np.arange(seq_total // GRID_W) - seq_total // GRID_W // 2).astype(np.float32)
    cols = (np.arange(GRID_W) - GRID_W // 2).astype(np.float32)
    sign = np.where((np.arange(head_dim) // quarter) % 2 == 0, -1.0, 1.0).astype(np.float32)

    def tables(positions):
        angle = np.tile((positions[:, None] * inverse[None, :]).astype(np.float32), (1, 4))
        angle = angle.astype(np.float64)
        return np.stack([np.cos(angle), np.sin(angle) * sign]).astype(np.float32)

    return tables(rows), tables(cols)


def ring_kernel(
    n_sp,
    n_tp,
    row_tab,
    col_tab,
    q_ref,
    k_ref,
    v_ref,
    qg_ref,
    kg_ref,
    res_ref,
    ow_ref,
    mg_ref,
    fg_ref,
    g_ref,
    u_ref,
    d_ref,
    cg_ref,
    cv_ref,
    out_ref,
    kv,
    q_rot,
    top,
    den,
    acc,
    att_own,
    att_all,
    ow_all,
    mix,
    stream,
    normed,
    wbuf,
    ups,
    hidden,
    part,
    red,
    kv_s,
    kv_r,
    sib_s,
    sib_r,
    w_s,
    w_r,
    y_s,
    y_r,
    ow_s,
    ow_r,
    nm_s,
    nm_r,
    a2a_s,
    a2a_r,
    halo_s,
    halo_r,
    red_s,
    red_r,
):
    half = n_sp // 2
    n_x = n_tp // 2
    tok = q_ref.shape[0]
    own = res_ref.shape[0]
    model = res_ref.shape[1]
    units = g_ref.shape[0]
    common = units // 3 // 16 * 16
    private = (units - common) // 2
    piece_tok = tok // 2
    sources = (g_ref, u_ref, d_ref)

    g = lax.axis_index("grp")
    s = lax.axis_index("sp")
    t = lax.axis_index("tp")
    x, c = t // 2, t % 2
    z_right, z_left = (s + 1) % n_sp, (s + n_sp - 1) % n_sp
    partner = g + 1 - 2 * (g % 2)
    sibling = t + 1 - 2 * c
    x_right = 2 * ((x + 1) % n_x) + c
    x_left = 2 * ((x + n_x - 1) % n_x) + c
    kv_head = t // (HEADS // KVH)

    barrier = pltpu.get_barrier_semaphore()
    peers = [{"sp": z_right}, {"sp": z_left}, {"grp": partner}]
    peers += [{"tp": (t + i) % n_tp} for i in range(1, n_tp)]
    for peer in peers:
        pl.semaphore_signal(barrier, inc=1, device_id=peer, device_id_type=MESH)

    def remote(src, dst, send, recv, device):
        return pltpu.make_async_remote_copy(
            src_ref=src,
            dst_ref=dst,
            send_sem=send,
            recv_sem=recv,
            device_id=device,
            device_id_type=MESH,
        )

    def block_of(direction, step):
        return (s + n_sp - step) % n_sp if direction == 0 else (s + step) % n_sp

    def z_device(direction):
        return {"sp": z_right if direction == 0 else z_left}

    def kv_at(which, block, piece):
        start = pl.multiple_of(block * tok + piece * piece_tok, piece_tok)
        return kv.at[which, pl.ds(start, piece_tok), :]

    def kv_copy(direction, step, piece, block):
        ref = kv_at(c, block, piece)
        i = (direction * half + step) * 2 + piece
        return remote(ref, ref, kv_s.at[i], kv_r.at[i], z_device(direction))

    def sib_copy(which, direction, step, piece, block):
        ref = kv_at(which, block, piece)
        i = (direction * half + step) * 2 + piece
        return remote(ref, ref, sib_s.at[i], sib_r.at[i], {"tp": sibling})

    def w_rows(piece):
        if piece == 0:
            return pl.ds(pl.multiple_of((g % 2) * (private + common), 16), private)
        return pl.ds(private, common)

    def w_at(a, block, rows):
        return wbuf.at[a, rows, pl.ds(pl.multiple_of(block * LANES, LANES), LANES)]

    def w_copy(a, direction, step, piece, block, first=False):
        rows = w_rows(piece)
        dst = w_at(a, block, rows)
        src = sources[a].at[rows, :] if first else dst
        i = ((a * 2 + direction) * half + step) * 2 + piece
        return remote(src, dst, w_s.at[i], w_r.at[i], z_device(direction))

    def y_copy(a, direction, step, block, mine):
        side = g % 2 if mine else 1 - g % 2
        rows = pl.ds(pl.multiple_of(side * (private + common), 16), private)
        ref = w_at(a, block, rows)
        i = (a * 2 + direction) * half + step
        return remote(ref, ref, y_s.at[i], y_r.at[i], {"grp": partner})

    def w_start(arrays):
        for piece in range(2):
            for a in arrays:
                for direction in range(2):
                    w_copy(a, direction, 0, piece, s, first=True).start()

    def when(condition):
        if isinstance(condition, bool):
            return (lambda f: f()) if condition else (lambda f: None)
        return pl.when(condition)

    def w_serve(arrays, k):
        for piece in range(2):
            for a in arrays:
                for direction in range(2):
                    last = direction == piece
                    block = block_of(direction, k)

                    @when(k <= half if last else k < half)
                    def _():
                        w_copy(a, direction, k - 1, piece, block).wait_recv()

                        @when(k <= half - 1 if last else k <= half - 2)
                        def _():
                            w_copy(a, direction, k, piece, block).start()

                        if piece == 0:
                            y_copy(a, direction, k - 1, block, True).start()

    def x_gather(buf, rows, first, send, recv):
        hold = rows // 2

        def at(block, lo, size):
            return buf.at[pl.ds(pl.multiple_of(block * rows + lo, 16), size), :]

        def ring(direction, step, chip, lo, size, src=None):
            dst = at(2 * chip + c, lo, size)
            i = direction * 2 + step
            device = {"tp": x_right if direction == 0 else x_left}
            return remote(dst if src is None else src, dst, send.at[i], recv.at[i], device)

        def share(i, chip, core, lo, size, src=None):
            dst = at(2 * chip + core, lo, size)
            return remote(
                dst if src is None else src, dst, send.at[4 + i], recv.at[4 + i], {"tp": sibling}
            )

        chips = ((x + n_x - 1) % n_x, (x + 1) % n_x)
        far = (x + 2) % n_x

        def start():
            for direction in range(2):
                ring(direction, 0, x, 0, rows, first).start()
            share(4, x, c, 0, rows, first).start()

        def middle():
            for direction in range(2):
                chip = chips[direction]
                ring(direction, 0, chip, 0, rows).wait_recv()
                ring(direction, 1, chip, direction * hold, hold).start()
                share(direction, chip, c, 0, rows).start()

        def end():
            for direction in range(2):
                ring(direction, 1, far, direction * hold, hold).wait_recv()
                share(2 + direction, far, c, direction * hold, hold).start()

        def arrived():
            other = 1 - c
            share(4, x, other, 0, rows).wait_recv()
            for direction in range(2):
                share(direction, chips[direction], other, 0, rows).wait_recv()
                share(2 + direction, far, other, direction * hold, hold).wait_recv()

        def sent():
            for direction in range(2):
                ring(direction, 0, x, 0, rows, first).wait_send()
                ring(direction, 1, chips[direction], direction * hold, hold).wait_send()
                share(direction, chips[direction], c, 0, rows).wait_send()
                share(2 + direction, far, c, direction * hold, hold).wait_send()
            share(4, x, c, 0, rows, first).wait_send()

        return start, middle, end, arrived, sent

    ow_start, ow_middle, ow_end, ow_arrived, ow_sent = x_gather(
        ow_all, ow_ref.shape[0], ow_ref, ow_s, ow_r
    )
    nm_start, nm_middle, nm_end, nm_arrived, nm_sent = x_gather(normed, own, None, nm_s, nm_r)

    grid_rows = tok // GRID_W
    lane = lax.broadcasted_iota(jnp.int32, (GRID_W, LANES), 1)
    quarter = LANES // 4

    def prepare(raw, gain, grid_row, factor):
        floats = raw.astype(F32)
        mean = jnp.sum(floats * floats, axis=-1, keepdims=True) * (1.0 / LANES)
        n = floats * lax.rsqrt(mean + EPSILON) * gain
        at = s * grid_rows + grid_row
        cos = jnp.where(lane < LANES // 2, row_tab[0, pl.ds(at, 1), :], col_tab[0])
        sin = jnp.where(lane < LANES // 2, row_tab[1, pl.ds(at, 1), :], col_tab[1])
        turned = jnp.where(
            (lane // quarter) % 2 == 0,
            pltpu.roll(n, LANES - quarter, 1),
            pltpu.roll(n, quarter, 1),
        )
        return ((n * cos + turned * sin) * factor).astype(BF16)

    head_cols = pl.ds(pl.multiple_of(kv_head * LANES, LANES), LANES)

    @pl.loop(0, grid_rows)
    def _(r):
        rows = pl.ds(pl.multiple_of(r * GRID_W, GRID_W), GRID_W)
        into = pl.ds(pl.multiple_of(s * tok + r * GRID_W, GRID_W), GRID_W)
        kv[0, into, :] = prepare(k_ref[rows, head_cols], kg_ref[...], r, 1.0)
        kv[1, into, :] = v_ref[rows, head_cols]

    pl.semaphore_wait(barrier, len(peers))
    for piece in range(2):
        for direction in range(2):
            kv_copy(direction, 0, piece, s).start()
    ow_start()

    @pl.loop(0, grid_rows)
    def _(r):
        rows = pl.ds(pl.multiple_of(r * GRID_W, GRID_W), GRID_W)
        q_rot[rows, :] = prepare(q_ref[rows, :], qg_ref[...], r, LANES ** (-0.5))

    top[...] = jnp.full_like(top, -1e30)
    den[...] = jnp.zeros_like(den)
    acc[...] = jnp.zeros_like(acc)
    for a in range(3):
        wbuf[a, :, pl.ds(pl.multiple_of(s * LANES, LANES), LANES)] = sources[a][...]
    ow_rows = ow_ref.shape[0]
    ow_all[pl.ds(pl.multiple_of(t * ow_rows, 16), ow_rows), :] = ow_ref[...]

    chunk = min(256, tok)

    def attend(block):
        keys = pl.ds(pl.multiple_of(block * tok, tok), tok)

        @pl.loop(0, tok // chunk)
        def _(i):
            rows = pl.ds(pl.multiple_of(i * chunk, chunk), chunk)
            scores = lax.dot_general(
                q_rot[rows, :],
                kv[0, keys, :],
                (((1,), (1,)), ((), ())),
                preferred_element_type=F32,
            )
            before = top[rows, :]
            newest = jnp.maximum(before, jnp.max(scores, axis=1, keepdims=True))
            wide = jnp.concatenate([newest] * (tok // LANES), axis=1)
            weights = jnp.exp(scores - wide)
            fade = jnp.exp(before - newest)
            den[rows, :] = den[rows, :] * fade + jnp.sum(weights, axis=1, keepdims=True)
            acc[rows, :] = acc[rows, :] * fade + jnp.dot(
                weights.astype(BF16), kv[1, keys, :], preferred_element_type=F32
            )
            top[rows, :] = newest

    @pl.loop(1, half + 2)
    def _(k):
        for piece in range(2):
            for direction in range(2):
                last = direction == piece
                block = block_of(direction, k)

                @pl.when(k <= half if last else k < half)
                def _():
                    kv_copy(direction, k - 1, piece, block).wait_recv()

                    @pl.when(k <= half - 1 if last else k <= half - 2)
                    def _():
                        kv_copy(direction, k, piece, block).start()

                    sib_copy(c, direction, k - 1, piece, block).start()

        @pl.when(k == half - 1)
        def _():
            w_start((0, 1))

        @pl.when(k == half // 2)
        def _():
            ow_middle()

        @pl.when(k == half - 1)
        def _():
            ow_end()

        for piece in range(2):
            for direction in range(2):
                last = direction == piece
                block = block_of(direction, k - 1)

                @pl.when((k >= 2) & (k <= half + 1 if last else k <= half))
                def _():
                    sib_copy(1 - c, direction, k - 2, piece, block).wait_recv()

        @pl.loop(0, jnp.where((k == 1) | (k == half + 1), 1, 2))
        def _(i):
            attend((s + n_sp + (k - 1) * (2 * i - 1)) % n_sp)

    w_serve((0, 1), 1)
    att_own[...] = (acc[...] / den[...]).astype(BF16)

    def att_copy(i, to, source):
        cols = pl.ds(pl.multiple_of(source * LANES, LANES), LANES)
        rows = pl.ds(pl.multiple_of(to * own, 16), own)
        return remote(
            att_own.at[rows, :],
            att_all.at[:, cols],
            a2a_s.at[i - 1],
            a2a_r.at[i - 1],
            {"tp": to},
        )

    for i in range(1, n_tp):
        att_copy(i, (t + i) % n_tp, t).start()
    att_all[:, pl.ds(pl.multiple_of(t * LANES, LANES), LANES)] = att_own[
        pl.ds(pl.multiple_of(t * own, 16), own), :
    ]
    ow_arrived()
    w_serve((0, 1), 2)
    for i in range(1, n_tp):
        att_copy(i, t, (t + n_tp - i) % n_tp).wait_recv()

    width = min(512, model)

    @pl.loop(0, model // width)
    def _(j):
        cols = pl.ds(pl.multiple_of(j * width, width), width)
        total = jnp.zeros((own, width), F32)
        for head in range(n_tp):
            span = slice(head * LANES, (head + 1) * LANES)
            total += (
                jnp.dot(att_all[:, span], ow_all[span, cols], preferred_element_type=F32)
                .astype(BF16)
                .astype(F32)
            )
        mix[:, cols] = total

    @pl.loop(0, own // 16)
    def _(r):
        rows = pl.ds(pl.multiple_of(r * 16, 16), 16)
        m = mix[rows, :]
        scale = lax.rsqrt(jnp.mean(m * m, axis=-1, keepdims=True) + EPSILON)
        added = (res_ref[rows, :].astype(F32) + m * scale * mg_ref[...]).astype(BF16)
        stream[rows, :] = added
        f = added.astype(F32)
        scale = lax.rsqrt(jnp.mean(f * f, axis=-1, keepdims=True) + EPSILON)
        normed[pl.ds(pl.multiple_of(t * own + r * 16, 16), 16), :] = (
            f * scale * fg_ref[...]
        ).astype(BF16)

    served = min(3, half)
    if served == 3:
        w_serve((0, 1), 3)
    nm_start()
    for k in range(served + 1, half + 1):
        w_serve((0, 1), k)
        if k == half - 1:
            w_start((2,))
        if k == served + 1:
            nm_middle()
        if k == served + 3:
            nm_end()
    if half < served + 1:
        w_start((2,))
        nm_middle()
        nm_end()
    elif half < served + 3:
        nm_end()
    nm_arrived()

    def y_arrived(a, direction, step):
        y_copy(a, direction, step, block_of(direction, step + 1), False).wait_recv()

    for a in range(2):
        for step in range(half):
            for direction in range(2 if step < half - 1 else 1):
                y_arrived(a, direction, step)

    m_rows = min(256, tok)
    m_count = tok // m_rows

    @pl.loop(0, m_count)
    def _(i):
        rows = pl.ds(pl.multiple_of(i * m_rows, m_rows), m_rows)
        for a in range(2):
            made = lax.dot_general(
                normed[rows, :],
                wbuf[a],
                (((1,), (1,)), ((), ())),
                preferred_element_type=F32,
            )
            ups[a, pl.ds(pl.multiple_of(8 + i * m_rows, 8), m_rows), :] = made.astype(BF16).astype(
                F32
            )

        @pl.when(i + 1 <= half)
        def _():
            w_serve((2,), i + 1)

    done = min(m_count, half)

    def halo_copy(direction):
        if direction == 0:
            src, dst = ups.at[:, pl.ds(tok, 8), :], ups.at[:, pl.ds(0, 8), :]
        else:
            src, dst = ups.at[:, pl.ds(8, 8), :], ups.at[:, pl.ds(tok + 8, 8), :]
        return remote(src, dst, halo_s.at[direction], halo_r.at[direction], z_device(direction))

    for direction in range(2):
        halo_copy(direction).start()

    c_rows = min(32, tok)
    c_count = tok // c_rows
    every = max(c_count // 4, 1)

    @pl.loop(0, c_count)
    def _(i):
        at = (i + 1) % c_count

        @pl.when(i == c_count - 2)
        def _():
            for direction in range(2):
                halo_copy(direction).wait_recv()
            ups[:, pl.ds(0, 8), :] = jnp.where(s == 0, 0.0, ups[:, pl.ds(0, 8), :])
            ups[:, pl.ds(tok + 8, 8), :] = jnp.where(
                s == n_sp - 1, 0.0, ups[:, pl.ds(tok + 8, 8), :]
            )

        mixed = []
        for a, taps in ((0, cg_ref), (1, cv_ref)):
            near = ups[a, pl.ds(pl.multiple_of(at * c_rows, c_rows), c_rows + 16), :]
            mixed.append(
                taps[0:1, :] * near[7 : 7 + c_rows]
                + taps[1:2, :] * near[8 : 8 + c_rows]
                + taps[2:3, :] * near[9 : 9 + c_rows]
            )
        v = mixed[0]
        inner = (2.0 / np.pi) ** 0.5 * (v + 0.044715 * (v * v * v))
        gated = 0.5 * v * (1.0 + jnp.tanh(inner)) * mixed[1]
        hidden[pl.ds(pl.multiple_of(at * c_rows, c_rows), c_rows), :] = gated.astype(BF16)

        @pl.when((i % every == every - 1) & (done + 1 + i // every <= half))
        def _():
            w_serve((2,), done + 1 + i // every)

    done = min(half, done + c_count // every)

    def red_copy(i, to, source, block):
        rows = pl.ds(pl.multiple_of(to * own, 16), own)
        return remote(
            part.at[block, rows, :],
            red.at[source, block],
            red_s.at[i - 1],
            red_r.at[i - 1],
            {"tp": to},
        )

    def red_all(i, source):
        return remote(
            red.at[source], red.at[source], red_s.at[i - 1], red_r.at[i - 1], {"tp": source}
        )

    @pl.loop(1, half + 1)
    def _(j):
        @pl.when(j > done)
        def _():
            w_serve((2,), j)

        y_arrived(2, 0, j - 1)

        @pl.when(j < half)
        def _():
            y_arrived(2, 1, j - 1)

        first, second = (s + n_sp - j) % n_sp, (s + j % half) % n_sp

        def cols(block):
            return pl.ds(pl.multiple_of(block * LANES, LANES), LANES)

        @pl.loop(0, m_count)
        def _(i):
            rows = pl.ds(pl.multiple_of(i * m_rows, m_rows), m_rows)
            both = jnp.concatenate([wbuf[2, :, cols(first)], wbuf[2, :, cols(second)]], axis=1)
            made = jnp.dot(hidden[rows, :], both, preferred_element_type=F32).astype(BF16)
            part[first, rows, :] = made[:, :LANES]
            part[second, rows, :] = made[:, LANES:]

        for i in range(1, n_tp):
            to = (t + i) % n_tp
            red_copy(i, to, t, first).start()
            red_copy(i, to, t, second).start()

    for i in range(1, n_tp):
        red_all(i, (t + n_tp - i) % n_tp).wait_recv()

    own_rows = pl.ds(pl.multiple_of(t * own, 16), own)
    for b in range(n_sp):
        span = slice(b * LANES, (b + 1) * LANES)
        total = part[b, own_rows, :].astype(F32)
        for i in range(1, n_tp):
            total += red[(t + n_tp - i) % n_tp, b].astype(F32)
        out_ref[:, span] = (stream[:, span].astype(F32) + total).astype(BF16)

    ow_sent()
    nm_sent()
    for i in range(1, n_tp):
        att_copy(i, (t + i) % n_tp, t).wait_send()
        red_all(i, (t + i) % n_tp).wait_send()
    for direction in range(2):
        halo_copy(direction).wait_send()
        for step in range(half):
            for piece in range(2):
                if step == half - 1 and direction != piece:
                    continue
                block = block_of(direction, step)
                kv_copy(direction, step, piece, block).wait_send()
                sib_copy(c, direction, step, piece, block_of(direction, step + 1)).wait_send()
                for a in range(3):
                    w_copy(a, direction, step, piece, block, first=step == 0).wait_send()
                    if piece == 0:
                        y_copy(
                            a, direction, step, block_of(direction, step + 1), True
                        ).wait_send()


def body(
    queries,
    keys,
    values,
    query_gain,
    key_gain,
    residual,
    out_weight,
    mix_gain,
    ffn_gain,
    gate_in,
    value_in,
    conv_gate,
    conv_value,
    down_t,
):
    n_sp, n_tp = lax.axis_size("sp"), lax.axis_size("tp")
    half = n_sp // 2
    tok = queries.shape[0]
    own, model = residual.shape
    units = gate_in.shape[1]
    row_tab, col_tab = rotary_tables(tok * n_sp, query_gain.shape[0])
    vmem = pl.BlockSpec(memory_space=pltpu.VMEM)
    dma = pltpu.SemaphoreType.DMA
    operands = (
        jnp.asarray(row_tab),
        jnp.asarray(col_tab),
        queries,
        keys,
        values,
        query_gain[None, :],
        key_gain[None, :],
        residual,
        out_weight,
        mix_gain[None, :],
        ffn_gain[None, :],
        gate_in.T,
        value_in.T,
        down_t.T,
        conv_gate,
        conv_value,
    )
    return pl.pallas_call(
        functools.partial(ring_kernel, n_sp, n_tp),
        out_shape=jax.ShapeDtypeStruct((own, model), BF16),
        in_specs=[vmem] * len(operands),
        out_specs=vmem,
        scratch_shapes=[
            pltpu.VMEM((2, tok * n_sp, LANES), BF16),
            pltpu.VMEM((tok, LANES), BF16),
            pltpu.VMEM((tok, LANES), F32),
            pltpu.VMEM((tok, LANES), F32),
            pltpu.VMEM((tok, LANES), F32),
            pltpu.VMEM((tok, LANES), BF16),
            pltpu.VMEM((own, n_tp * LANES), BF16),
            pltpu.VMEM((n_tp * out_weight.shape[0], model), BF16),
            pltpu.VMEM((own, model), F32),
            pltpu.VMEM((own, model), BF16),
            pltpu.VMEM((tok, model), BF16),
            pltpu.VMEM((3, units, model), BF16),
            pltpu.VMEM((2, tok + 16, units), F32),
            pltpu.VMEM((tok, units), BF16),
            pltpu.VMEM((n_sp, tok, LANES), BF16),
            pltpu.VMEM((n_tp, n_sp, own, LANES), BF16),
            dma((4 * half,)),
            dma((4 * half,)),
            dma((4 * half,)),
            dma((4 * half,)),
            dma((12 * half,)),
            dma((12 * half,)),
            dma((6 * half,)),
            dma((6 * half,)),
            dma((9,)),
            dma((9,)),
            dma((9,)),
            dma((9,)),
            dma((n_tp - 1,)),
            dma((n_tp - 1,)),
            dma((2,)),
            dma((2,)),
            dma((n_tp - 1,)),
            dma((n_tp - 1,)),
        ],
        compiler_params=pltpu.CompilerParams(
            collective_id=0,
            has_side_effects=True,
            vmem_limit_bytes=62 * 1024 * 1024,
        ),
        name="layer",
    )(*operands)


def solution(mesh):
    return jax.shard_map(
        body,
        mesh=mesh,
        in_specs=(
            P(("grp", "sp"), "tp"),
            P(("grp", "sp"), None),
            P(("grp", "sp"), None),
            P(),
            P(),
            P(("grp", "sp", "tp"), None),
            P("tp", None),
            P(),
            P(),
            P("sp", "tp"),
            P("sp", "tp"),
            P(None, "tp"),
            P(None, "tp"),
            P("sp", "tp"),
        ),
        out_specs=P(("grp", "sp", "tp"), None),
        check_vma=False,
    )
```

```python
import functools

import jax
import jax.numpy as jnp
import numpy as np
from jax import lax
from jax.experimental import pallas as pl
from jax.experimental.pallas import tpu as pltpu
from jax.sharding import PartitionSpec as P

HEADS = 8
KVH = 2
GRID_W = 64
EPSILON = 1e-06
THETA = 10000.0
LANES = 128
MESH = pl.DeviceIdType.MESH
F32 = jnp.float32
BF16 = jnp.bfloat16


def rotary_tables(seq_total, head_dim):
    quarter = head_dim // 4
    inverse = np.float32(THETA) ** (
        -(np.float32(2.0) * np.arange(quarter, dtype=np.float32)) / np.float32(head_dim // 2)
    )
    inverse = inverse.astype(np.float32)
    rows = (np.arange(seq_total // GRID_W) - seq_total // GRID_W // 2).astype(np.float32)
    cols = (np.arange(GRID_W) - GRID_W // 2).astype(np.float32)
    sign = np.where((np.arange(head_dim) // quarter) % 2 == 0, -1.0, 1.0).astype(np.float32)

    def tables(positions):
        angle = np.tile((positions[:, None] * inverse[None, :]).astype(np.float32), (1, 4))
        angle = angle.astype(np.float64)
        return np.stack([np.cos(angle), np.sin(angle) * sign]).astype(np.float32)

    return tables(rows), tables(cols)


def ring_kernel(
    n_sp,
    n_tp,
    row_tab,
    col_tab,
    q_ref,
    k_ref,
    v_ref,
    qg_ref,
    kg_ref,
    res_ref,
    ow_ref,
    mg_ref,
    fg_ref,
    g_ref,
    u_ref,
    d_ref,
    cg_ref,
    cv_ref,
    out_ref,
    kv,
    q_rot,
    top,
    den,
    acc,
    att_own,
    att_all,
    ow_all,
    mix,
    stream,
    normed,
    wbuf,
    ups,
    hidden,
    part,
    pair_in,
    pair_sum,
    far_in,
    near_in,
    kv_s,
    kv_r,
    sib_s,
    sib_r,
    xp_s,
    xp_r,
    rel_s,
    rel_r,
    w_s,
    w_r,
    y_s,
    y_r,
    ow_s,
    ow_r,
    nm_s,
    nm_r,
    a2a_s,
    a2a_r,
    halo_s,
    halo_r,
    pair_s,
    pair_r,
    far_s,
    far_r,
    near_s,
    near_r,
):
    half = n_sp // 2
    n_x = n_tp // 2
    tok = q_ref.shape[0]
    own = res_ref.shape[0]
    model = res_ref.shape[1]
    units = g_ref.shape[0]
    common = units // 3 // 16 * 16
    private = (units - common) // 2
    kv_common = tok // 3 // 32 * 32
    kv_private = (tok - kv_common) // 2
    sources = (g_ref, u_ref, d_ref)

    g = lax.axis_index("grp")
    s = lax.axis_index("sp")
    t = lax.axis_index("tp")
    x, c = t // 2, t % 2
    z_right, z_left = (s + 1) % n_sp, (s + n_sp - 1) % n_sp
    partner = g + 1 - 2 * (g % 2)
    sibling = t + 1 - 2 * c
    x_right = 2 * ((x + 1) % n_x) + c
    x_left = 2 * ((x + n_x - 1) % n_x) + c
    kv_head = t // (HEADS // KVH)
    x_pair = x + 1 - 2 * (x % 2)
    x_cross = (x + n_x - 1 + 2 * (x % 2)) % n_x

    barrier = pltpu.get_barrier_semaphore()
    peers = [{"sp": z_right}, {"sp": z_left}, {"grp": partner}]
    peers += [{"tp": (t + i) % n_tp} for i in range(1, n_tp)]
    for peer in peers:
        pl.semaphore_signal(barrier, inc=1, device_id=peer, device_id_type=MESH)

    def remote(src, dst, send, recv, device):
        return pltpu.make_async_remote_copy(
            src_ref=src,
            dst_ref=dst,
            send_sem=send,
            recv_sem=recv,
            device_id=device,
            device_id_type=MESH,
        )

    def block_of(direction, step):
        return (s + n_sp - step) % n_sp if direction == 0 else (s + step) % n_sp

    def z_device(direction):
        return {"sp": z_right if direction == 0 else z_left}

    def kv_at(which, block, piece, side):
        if piece == 0:
            start, size = side * (kv_private + kv_common), kv_private
        else:
            start, size = kv_private, kv_common
        return kv.at[which, pl.ds(pl.multiple_of(block * tok + start, 16), size), :]

    def kv_copy(direction, step, piece, block):
        ref = kv_at(c, block, piece, x % 2)
        i = (direction * half + step) * 2 + piece
        return remote(ref, ref, kv_s.at[i], kv_r.at[i], z_device(direction))

    def sib_copy(which, direction, step, piece, block):
        ref = kv_at(which, block, piece, x % 2)
        i = (direction * half + step) * 2 + piece
        return remote(ref, ref, sib_s.at[i], sib_r.at[i], {"tp": sibling})

    def xp_copy(direction, step, block, mine):
        ref = kv_at(c, block, 0, x % 2 if mine else 1 - x % 2)
        i = direction * half + step
        return remote(ref, ref, xp_s.at[i], xp_r.at[i], {"tp": 2 * x_pair + c})

    def rel_copy(which, direction, step, block):
        ref = kv_at(which, block, 0, 1 - x % 2)
        i = direction * half + step
        return remote(ref, ref, rel_s.at[i], rel_r.at[i], {"tp": sibling})

    def w_rows(piece):
        if piece == 0:
            return pl.ds(pl.multiple_of((g % 2) * (private + common), 16), private)
        return pl.ds(private, common)

    def w_at(a, block, rows):
        return wbuf.at[a, rows, pl.ds(pl.multiple_of(block * LANES, LANES), LANES)]

    def w_copy(a, direction, step, piece, block, first=False):
        rows = w_rows(piece)
        dst = w_at(a, block, rows)
        src = sources[a].at[rows, :] if first else dst
        i = ((a * 2 + direction) * half + step) * 2 + piece
        return remote(src, dst, w_s.at[i], w_r.at[i], z_device(direction))

    def y_copy(a, direction, step, block, mine):
        side = g % 2 if mine else 1 - g % 2
        rows = pl.ds(pl.multiple_of(side * (private + common), 16), private)
        ref = w_at(a, block, rows)
        i = (a * 2 + direction) * half + step
        return remote(ref, ref, y_s.at[i], y_r.at[i], {"grp": partner})

    def w_start(arrays):
        for piece in range(2):
            for a in arrays:
                for direction in range(2):
                    w_copy(a, direction, 0, piece, s, first=True).start()

    def when(condition):
        if isinstance(condition, bool):
            return (lambda f: f()) if condition else (lambda f: None)
        return pl.when(condition)

    def w_serve(arrays, k, pieces=(0, 1)):
        for piece in pieces:
            for a in arrays:
                for direction in range(2):
                    last = direction == piece
                    block = block_of(direction, k)

                    @when((k >= 1) & (k <= half if last else k < half))
                    def _():
                        w_copy(a, direction, k - 1, piece, block).wait_recv()

                        @when(k <= half - 1 if last else k <= half - 2)
                        def _():
                            w_copy(a, direction, k, piece, block).start()

                        if piece == 0:
                            y_copy(a, direction, k - 1, block, True).start()

    def x_gather(buf, rows, first, send, recv):
        hold = rows // 2

        def at(block, lo, size):
            return buf.at[pl.ds(pl.multiple_of(block * rows + lo, 16), size), :]

        def ring(direction, step, chip, lo, size, src=None):
            dst = at(2 * chip + c, lo, size)
            i = direction * 2 + step
            device = {"tp": x_right if direction == 0 else x_left}
            return remote(dst if src is None else src, dst, send.at[i], recv.at[i], device)

        def share(i, chip, core, lo, size, src=None):
            dst = at(2 * chip + core, lo, size)
            return remote(
                dst if src is None else src, dst, send.at[4 + i], recv.at[4 + i], {"tp": sibling}
            )

        chips = ((x + n_x - 1) % n_x, (x + 1) % n_x)
        far = (x + 2) % n_x

        def start():
            for direction in range(2):
                ring(direction, 0, x, 0, rows, first).start()
            share(4, x, c, 0, rows, first).start()

        def middle():
            for direction in range(2):
                chip = chips[direction]
                ring(direction, 0, chip, 0, rows).wait_recv()
                ring(direction, 1, chip, direction * hold, hold).start()
                share(direction, chip, c, 0, rows).start()

        def end():
            for direction in range(2):
                ring(direction, 1, far, direction * hold, hold).wait_recv()
                share(2 + direction, far, c, direction * hold, hold).start()

        def arrived():
            other = 1 - c
            share(4, x, other, 0, rows).wait_recv()
            for direction in range(2):
                share(direction, chips[direction], other, 0, rows).wait_recv()
                share(2 + direction, far, other, direction * hold, hold).wait_recv()

        def sent():
            for direction in range(2):
                ring(direction, 0, x, 0, rows, first).wait_send()
                ring(direction, 1, chips[direction], direction * hold, hold).wait_send()
                share(direction, chips[direction], c, 0, rows).wait_send()
                share(2 + direction, far, c, direction * hold, hold).wait_send()
            share(4, x, c, 0, rows, first).wait_send()

        return start, middle, end, arrived, sent

    ow_rows = ow_ref.shape[0]
    ow_parts = 4
    ow_far = x_cross + 1 - 2 * (x_cross % 2)

    def ow_copy(i, chip, core, lo, size, device, first=False):
        dst = ow_all.at[pl.ds(pl.multiple_of((2 * chip + core) * ow_rows + lo, 16), size), :]
        src = ow_ref.at[pl.ds(lo, size), :] if first else dst
        return remote(src, dst, ow_s.at[i], ow_r.at[i], {"tp": device})

    size = ow_rows // ow_parts

    def ow_pair(q, chip, first=False):
        return ow_copy(q, chip, c, q * size, size, 2 * x_pair + c, first)

    def ow_over(chip, first=False):
        return ow_copy(4, chip, c, 0, ow_rows, 2 * x_cross + c, first)

    def ow_on(q, chip):
        return ow_copy(5 + q, chip, c, q * size, size, 2 * x_cross + c)

    def ow_own(core, first=False):
        return ow_copy(9, x, core, 0, ow_rows, sibling, first)

    def ow_share(i, chip, core, lo, size):
        return ow_copy(10 + i, chip, core, lo, size, sibling)

    def ow_shares(core, i):
        if i == 4:
            return ow_share(4, x_cross, core, 0, ow_rows)
        if i < 4:
            return ow_share(i, x_pair, core, i * size, size)
        return ow_share(i, ow_far, core, (i - 5) * size, size)

    def ow_take(q):
        ow_pair(q, x_pair).wait_recv()
        ow_on(q, x_pair).start()
        ow_shares(c, q).start()

    def ow_across():
        ow_over(x_cross).wait_recv()
        ow_shares(c, 4).start()

    def ow_take_far(q):
        ow_on(q, ow_far).wait_recv()
        ow_shares(c, 5 + q).start()

    nm_start, nm_middle, nm_end, nm_arrived, nm_sent = x_gather(normed, own, None, nm_s, nm_r)

    grid_rows = tok // GRID_W
    lane = lax.broadcasted_iota(jnp.int32, (GRID_W, LANES), 1)
    quarter = LANES // 4

    def prepare(raw, gain, grid_row, factor):
        floats = raw.astype(F32)
        mean = jnp.sum(floats * floats, axis=-1, keepdims=True) * (1.0 / LANES)
        n = floats * lax.rsqrt(mean + EPSILON) * gain
        at = s * grid_rows + grid_row
        cos = jnp.where(lane < LANES // 2, row_tab[0, pl.ds(at, 1), :], col_tab[0])
        sin = jnp.where(lane < LANES // 2, row_tab[1, pl.ds(at, 1), :], col_tab[1])
        turned = jnp.where(
            (lane // quarter) % 2 == 0,
            pltpu.roll(n, LANES - quarter, 1),
            pltpu.roll(n, quarter, 1),
        )
        return ((n * cos + turned * sin) * factor).astype(BF16)

    head_cols = pl.ds(pl.multiple_of(kv_head * LANES, LANES), LANES)

    @pl.loop(0, grid_rows)
    def _(r):
        rows = pl.ds(pl.multiple_of(r * GRID_W, GRID_W), GRID_W)
        into = pl.ds(pl.multiple_of(s * tok + r * GRID_W, GRID_W), GRID_W)
        kv[0, into, :] = prepare(k_ref[rows, head_cols], kg_ref[...], r, 1.0)
        kv[1, into, :] = v_ref[rows, head_cols]

    pl.semaphore_wait(barrier, len(peers))
    for piece in range(2):
        for direction in range(2):
            kv_copy(direction, 0, piece, s).start()
    ow_over(x, first=True).start()
    ow_own(c, first=True).start()
    w_start((0,))

    @pl.loop(0, grid_rows)
    def _(r):
        rows = pl.ds(pl.multiple_of(r * GRID_W, GRID_W), GRID_W)
        q_rot[rows, :] = prepare(q_ref[rows, :], qg_ref[...], r, LANES ** (-0.5))

    top[...] = jnp.full_like(top, -1e30)
    den[...] = jnp.zeros_like(den)
    acc[...] = jnp.zeros_like(acc)
    for a in range(3):
        wbuf[a, :, pl.ds(pl.multiple_of(s * LANES, LANES), LANES)] = sources[a][...]
    ow_all[pl.ds(pl.multiple_of(t * ow_rows, 16), ow_rows), :] = ow_ref[...]

    chunk = min(256, tok)

    def attend(block):
        keys = pl.ds(pl.multiple_of(block * tok, tok), tok)

        @pl.loop(0, tok // chunk, unroll=True)
        def _(i):
            rows = pl.ds(pl.multiple_of(i * chunk, chunk), chunk)
            scores = lax.dot_general(
                q_rot[rows, :],
                kv[0, keys, :],
                (((1,), (1,)), ((), ())),
                preferred_element_type=F32,
            )
            before = top[rows, :]
            newest = jnp.maximum(before, jnp.max(scores, axis=1, keepdims=True))
            wide = jnp.concatenate([newest] * (tok // LANES), axis=1)
            weights = jnp.exp(scores - wide)
            fade = jnp.exp(before - newest)
            den[rows, :] = den[rows, :] * fade + jnp.sum(weights, axis=1, keepdims=True)
            acc[rows, :] = acc[rows, :] * fade + jnp.dot(
                weights.astype(BF16), kv[1, keys, :], preferred_element_type=F32
            )
            top[rows, :] = newest

    @pl.loop(1, half + 3)
    def _(k):
        def at_step(step, act):
            @pl.when(k == min(step, half + 2))
            def _():
                act()

        def kv_serve(piece):
            for direction in range(2):
                last = direction == piece
                block = block_of(direction, k)

                @pl.when(k <= half if last else k < half)
                def _():
                    kv_copy(direction, k - 1, piece, block).wait_recv()

                    @pl.when(k <= half - 1 if last else k <= half - 2)
                    def _():
                        kv_copy(direction, k, piece, block).start()

                    if piece == 0:
                        xp_copy(direction, k - 1, block, True).start()
                    sib_copy(c, direction, k - 1, piece, block).start()

        kv_serve(0)
        for q in range(ow_parts):
            at_step(1 + q, lambda: ow_pair(q, x, first=True).start())
        w_serve((0,), k - 1, (0,))
        for direction in range(2):
            block = block_of(direction, k - 1)

            @pl.when((k >= 2) & (k <= half + 1 if direction == 0 else k <= half))
            def _():
                xp_copy(direction, k - 2, block, False).wait_recv()
                rel_copy(c, direction, k - 2, block).start()

        for direction in range(2):
            block = block_of(direction, k - 2)
            for piece in range(2):
                last = direction == piece

                @pl.when((k >= 3) & (k <= half + 2 if last else k <= half + 1))
                def _():
                    sib_copy(1 - c, direction, k - 3, piece, block).wait_recv()

            @pl.when((k >= 3) & (k <= half + 2 if direction == 0 else k <= half + 1))
            def _():
                rel_copy(1 - c, direction, k - 3, block).wait_recv()

        @pl.when(k != 2)
        def _():
            attend((s + n_sp - jnp.where(k == 1, 0, k - 2)) % n_sp)

        kv_serve(1)
        w_serve((0,), k - 1, (1,))
        for q in range(ow_parts):
            at_step(3 + q, lambda: ow_take(q))
        at_step(5, ow_across)
        for q in range(ow_parts):
            at_step(7 + q, lambda: ow_take_far(q))
        at_step(half, lambda: w_start((1,)))

        @pl.when((k >= 3) & (k <= half + 1))
        def _():
            attend((s + k - 2) % n_sp)

        at_step(half + 2, lambda: w_serve((1,), 1))

    def vd_serve(k):
        for piece in range(2):
            w_serve((1,), k, (piece,))
            w_serve((2,), k - 2, (piece,))
        if k == 2:
            w_start((2,))

    att_own[...] = (acc[...] / den[...]).astype(BF16)

    def att_copy(i, to, source):
        cols = pl.ds(pl.multiple_of(source * LANES, LANES), LANES)
        rows = pl.ds(pl.multiple_of(to * own, 16), own)
        return remote(
            att_own.at[rows, :],
            att_all.at[:, cols],
            a2a_s.at[i - 1],
            a2a_r.at[i - 1],
            {"tp": to},
        )

    for i in range(1, n_tp):
        att_copy(i, (t + i) % n_tp, t).start()
    att_all[:, pl.ds(pl.multiple_of(t * LANES, LANES), LANES)] = att_own[
        pl.ds(pl.multiple_of(t * own, 16), own), :
    ]
    for i in range(2 * ow_parts + 1):
        ow_shares(1 - c, i).wait_recv()
    ow_own(1 - c).wait_recv()
    vd_serve(2)
    for i in range(1, n_tp):
        att_copy(i, t, (t + n_tp - i) % n_tp).wait_recv()

    width = min(512, model)

    @pl.loop(0, model // width)
    def _(j):
        cols = pl.ds(pl.multiple_of(j * width, width), width)
        total = jnp.zeros((own, width), F32)
        for head in range(n_tp):
            span = slice(head * LANES, (head + 1) * LANES)
            total += (
                jnp.dot(att_all[:, span], ow_all[span, cols], preferred_element_type=F32)
                .astype(BF16)
                .astype(F32)
            )
        mix[:, cols] = total

    @pl.loop(0, own // 16)
    def _(r):
        rows = pl.ds(pl.multiple_of(r * 16, 16), 16)
        m = mix[rows, :]
        scale = lax.rsqrt(jnp.mean(m * m, axis=-1, keepdims=True) + EPSILON)
        added = (res_ref[rows, :].astype(F32) + m * scale * mg_ref[...]).astype(BF16)
        stream[rows, :] = added
        f = added.astype(F32)
        scale = lax.rsqrt(jnp.mean(f * f, axis=-1, keepdims=True) + EPSILON)
        normed[pl.ds(pl.multiple_of(t * own + r * 16, 16), 16), :] = (
            f * scale * fg_ref[...]
        ).astype(BF16)

    vd_serve(3)
    nm_start()
    vd_serve(4)
    vd_serve(5)
    nm_middle()
    vd_serve(6)
    nm_end()
    vd_serve(7)
    nm_arrived()

    def y_arrived(a, direction, step):
        y_copy(a, direction, step, block_of(direction, step + 1), False).wait_recv()

    def y_all(a):
        for step in range(half):
            for direction in range(2 if step < half - 1 else 1):
                y_arrived(a, direction, step)

    m_rows = min(256, tok)
    m_count = tok // m_rows

    def up(a, i):
        rows = pl.ds(pl.multiple_of(i * m_rows, m_rows), m_rows)
        made = lax.dot_general(
            normed[rows, :], wbuf[a], (((1,), (1,)), ((), ())), preferred_element_type=F32
        )
        ups[a, pl.ds(pl.multiple_of(8 + i * m_rows, 8), m_rows), :] = made.astype(BF16).astype(F32)

    y_all(0)

    @pl.loop(0, m_count)
    def _(i):
        up(0, i)

    for k in range(8, half + 1):
        vd_serve(k)
    done = min(max(half, 7) - 2, half)
    y_all(1)

    @pl.loop(0, m_count)
    def _(i):
        up(1, i)

        @pl.when(done + 1 + i <= half)
        def _():
            w_serve((2,), done + 1 + i)

    done = min(done + m_count, half)

    def halo_copy(direction):
        if direction == 0:
            src, dst = ups.at[:, pl.ds(tok, 8), :], ups.at[:, pl.ds(0, 8), :]
        else:
            src, dst = ups.at[:, pl.ds(8, 8), :], ups.at[:, pl.ds(tok + 8, 8), :]
        return remote(src, dst, halo_s.at[direction], halo_r.at[direction], z_device(direction))

    for direction in range(2):
        halo_copy(direction).start()

    c_rows = min(32, own)

    def by_core(row):
        to = row // own
        start = ((to % 2) * n_x + to // 2) * own + row % own
        return pl.ds(pl.multiple_of(start, c_rows), c_rows)

    c_count = tok // c_rows
    every = max(c_count // 4, 1)

    @pl.loop(0, c_count)
    def _(i):
        at = (i + 1) % c_count

        @pl.when(i == c_count - 2)
        def _():
            for direction in range(2):
                halo_copy(direction).wait_recv()
            ups[:, pl.ds(0, 8), :] = jnp.where(s == 0, 0.0, ups[:, pl.ds(0, 8), :])
            ups[:, pl.ds(tok + 8, 8), :] = jnp.where(
                s == n_sp - 1, 0.0, ups[:, pl.ds(tok + 8, 8), :]
            )

        mixed = []
        for a, taps in ((0, cg_ref), (1, cv_ref)):
            near = ups[a, pl.ds(pl.multiple_of(at * c_rows, c_rows), c_rows + 16), :]
            mixed.append(
                taps[0:1, :] * near[7 : 7 + c_rows]
                + taps[1:2, :] * near[8 : 8 + c_rows]
                + taps[2:3, :] * near[9 : 9 + c_rows]
            )
        v = mixed[0]
        inner = (2.0 / np.pi) ** 0.5 * (v + 0.044715 * (v * v * v))
        gated = 0.5 * v * (1.0 + jnp.tanh(inner)) * mixed[1]
        hidden[by_core(at * c_rows), :] = gated.astype(BF16)

        @pl.when((i % every == every - 1) & (done + 1 + i // every <= half))
        def _():
            w_serve((2,), done + 1 + i // every)

    done = min(half, done + c_count // every)

    per_core = n_x * own
    cut = own // 2
    chip_right, chip_left = (x + 1) % n_x, (x + n_x - 1) % n_x
    chip_far = (x + 2) % n_x

    def pair_copy(i, block, core):
        rows = pl.ds(pl.multiple_of(core * per_core, 16), per_core)
        return remote(
            part.at[block, rows, :],
            pair_in.at[block],
            pair_s.at[i],
            pair_r.at[i],
            {"tp": sibling},
        )

    def far_copy(direction, block):
        lo = cut if direction == 0 else 0
        return remote(
            pair_sum.at[block, pl.ds(pl.multiple_of(chip_far * own + lo, 16), cut), :],
            far_in.at[direction, block],
            far_s.at[direction * n_sp + block],
            far_r.at[direction * n_sp + block],
            {"tp": x_right if direction == 0 else x_left},
        )

    def near_copy(direction, block):
        chip = chip_right if direction == 0 else chip_left
        return remote(
            pair_sum.at[block, pl.ds(pl.multiple_of(chip * own, 16), own), :],
            near_in.at[direction, block],
            near_s.at[direction],
            near_r.at[direction],
            {"tp": x_right if direction == 0 else x_left},
        )

    def near_all(direction):
        ref = near_in.at[direction]
        return remote(
            ref,
            ref,
            near_s.at[direction],
            near_r.at[direction],
            {"tp": x_right if direction == 0 else x_left},
        )

    def of_core(chip, size, lo=0):
        return pl.ds(pl.multiple_of(c * per_core + chip * own + lo, 16), size)

    def of_chip(chip, size, lo=0):
        return pl.ds(pl.multiple_of(chip * own + lo, 16), size)

    def blocks(j):
        return (s + n_sp - j) % n_sp, (s + j % half) % n_sp

    @pl.loop(1, half + 3)
    def _(j):
        @pl.when(j <= half)
        def _():
            @pl.when(j > done)
            def _():
                w_serve((2,), j)

            y_arrived(2, 0, j - 1)

            @pl.when(j < half)
            def _():
                y_arrived(2, 1, j - 1)

            first, second = blocks(j)

            def cols(block):
                return pl.ds(pl.multiple_of(block * LANES, LANES), LANES)

            @pl.loop(0, m_count)
            def _(i):
                rows = pl.ds(pl.multiple_of(i * m_rows, m_rows), m_rows)
                both = jnp.concatenate([wbuf[2, :, cols(first)], wbuf[2, :, cols(second)]], axis=1)
                made = jnp.dot(hidden[rows, :], both, preferred_element_type=F32).astype(BF16)
                part[first, rows, :] = made[:, :LANES]
                part[second, rows, :] = made[:, LANES:]

            for i, block in enumerate((first, second)):
                pair_copy(2 * (j - 1) + i, block, 1 - c).start()

        @pl.when((j >= 2) & (j <= half + 1))
        def _():
            for i, block in enumerate(blocks(j - 1)):
                pair_copy(2 * (j - 2) + i, block, c).wait_recv()
                for chip in (chip_far, chip_right, chip_left):
                    pair_sum[block, of_chip(chip, own), :] = (
                        part[block, of_core(chip, own), :].astype(F32)
                        + pair_in[block, of_chip(chip, own), :].astype(F32)
                    ).astype(BF16)
                for direction in range(2):
                    far_copy(direction, block).start()

        @pl.when(j >= 3)
        def _():
            for block in blocks(j - 2):
                for direction in range(2):
                    far_copy(direction, block).wait_recv()
                    chip = chip_right if direction == 0 else chip_left
                    lo = cut if direction == 0 else 0
                    pair_sum[block, of_chip(chip, cut, lo), :] = (
                        part[block, of_core(chip, cut, lo), :].astype(F32)
                        + pair_in[block, of_chip(chip, cut, lo), :].astype(F32)
                        + far_in[direction, block].astype(F32)
                    ).astype(BF16)
                    near_copy(direction, block).start()

    for direction in range(2):
        near_all(direction).wait_recv()

    for b in range(n_sp):
        span = slice(b * LANES, (b + 1) * LANES)
        total = part[b, of_core(x, own), :].astype(F32) + pair_in[b, of_chip(x, own), :].astype(F32)
        for direction in range(2):
            total += near_in[direction, b].astype(F32)
        out_ref[:, span] = (stream[:, span].astype(F32) + total).astype(BF16)

    for q in range(ow_parts):
        ow_pair(q, x, first=True).wait_send()
        ow_on(q, x_pair).wait_send()
    ow_over(x, first=True).wait_send()
    for i in range(2 * ow_parts + 1):
        ow_shares(c, i).wait_send()
    ow_own(c, first=True).wait_send()
    nm_sent()
    for i in range(1, n_tp):
        att_copy(i, (t + i) % n_tp, t).wait_send()
    for b in range(n_sp):
        pair_copy(b, b, 1 - c).wait_send()
        for direction in range(2):
            far_copy(direction, b).wait_send()
    for direction in range(2):
        near_all(direction).wait_send()
        halo_copy(direction).wait_send()
        for step in range(half):
            for piece in range(2):
                if step == half - 1 and direction != piece:
                    continue
                block = block_of(direction, step)
                kv_copy(direction, step, piece, block).wait_send()
                sib_copy(c, direction, step, piece, block_of(direction, step + 1)).wait_send()
                if piece == 0:
                    arriving = block_of(direction, step + 1)
                    xp_copy(direction, step, arriving, True).wait_send()
                    rel_copy(c, direction, step, arriving).wait_send()
                for a in range(3):
                    w_copy(a, direction, step, piece, block, first=step == 0).wait_send()
                    if piece == 0:
                        y_copy(
                            a, direction, step, block_of(direction, step + 1), True
                        ).wait_send()


def body(
    queries,
    keys,
    values,
    query_gain,
    key_gain,
    residual,
    out_weight,
    mix_gain,
    ffn_gain,
    gate_in,
    value_in,
    conv_gate,
    conv_value,
    down_t,
):
    n_sp, n_tp = lax.axis_size("sp"), lax.axis_size("tp")
    half = n_sp // 2
    tok = queries.shape[0]
    own, model = residual.shape
    units = gate_in.shape[1]
    row_tab, col_tab = rotary_tables(tok * n_sp, query_gain.shape[0])
    vmem = pl.BlockSpec(memory_space=pltpu.VMEM)
    dma = pltpu.SemaphoreType.DMA
    operands = (
        jnp.asarray(row_tab),
        jnp.asarray(col_tab),
        queries,
        keys,
        values,
        query_gain[None, :],
        key_gain[None, :],
        residual,
        out_weight,
        mix_gain[None, :],
        ffn_gain[None, :],
        gate_in.T,
        value_in.T,
        down_t.T,
        conv_gate,
        conv_value,
    )
    return pl.pallas_call(
        functools.partial(ring_kernel, n_sp, n_tp),
        out_shape=jax.ShapeDtypeStruct((own, model), BF16),
        in_specs=[vmem] * len(operands),
        out_specs=vmem,
        scratch_shapes=[
            pltpu.VMEM((2, tok * n_sp, LANES), BF16),
            pltpu.VMEM((tok, LANES), BF16),
            pltpu.VMEM((tok, LANES), F32),
            pltpu.VMEM((tok, LANES), F32),
            pltpu.VMEM((tok, LANES), F32),
            pltpu.VMEM((tok, LANES), BF16),
            pltpu.VMEM((own, n_tp * LANES), BF16),
            pltpu.VMEM((n_tp * out_weight.shape[0], model), BF16),
            pltpu.VMEM((own, model), F32),
            pltpu.VMEM((own, model), BF16),
            pltpu.VMEM((tok, model), BF16),
            pltpu.VMEM((3, units, model), BF16),
            pltpu.VMEM((2, tok + 16, units), F32),
            pltpu.VMEM((tok, units), BF16),
            pltpu.VMEM((n_sp, tok, LANES), BF16),
            pltpu.VMEM((n_sp, tok // 2, LANES), BF16),
            pltpu.VMEM((n_sp, tok // 2, LANES), BF16),
            pltpu.VMEM((2, n_sp, own // 2, LANES), BF16),
            pltpu.VMEM((2, n_sp, own, LANES), BF16),
            dma((4 * half,)),
            dma((4 * half,)),
            dma((4 * half,)),
            dma((4 * half,)),
            dma((2 * half,)),
            dma((2 * half,)),
            dma((2 * half,)),
            dma((2 * half,)),
            dma((12 * half,)),
            dma((12 * half,)),
            dma((6 * half,)),
            dma((6 * half,)),
            dma((19,)),
            dma((19,)),
            dma((9,)),
            dma((9,)),
            dma((n_tp - 1,)),
            dma((n_tp - 1,)),
            dma((2,)),
            dma((2,)),
            dma((n_sp,)),
            dma((n_sp,)),
            dma((2 * n_sp,)),
            dma((2 * n_sp,)),
            dma((2,)),
            dma((2,)),
        ],
        compiler_params=pltpu.CompilerParams(
            collective_id=0,
            has_side_effects=True,
            vmem_limit_bytes=62 * 1024 * 1024,
        ),
        name="layer",
    )(*operands)


def solution(mesh):
    return jax.shard_map(
        body,
        mesh=mesh,
        in_specs=(
            P(("grp", "sp"), "tp"),
            P(("grp", "sp"), None),
            P(("grp", "sp"), None),
            P(),
            P(),
            P(("grp", "sp", "tp"), None),
            P("tp", None),
            P(),
            P(),
            P("sp", "tp"),
            P("sp", "tp"),
            P(None, "tp"),
            P(None, "tp"),
            P("sp", "tp"),
        ),
        out_specs=P(("grp", "sp", "tp"), None),
        check_vma=False,
    )
```

```python
import functools

import jax
import jax.numpy as jnp
import numpy as np
from jax import lax
from jax.experimental import pallas as pl
from jax.experimental.pallas import tpu as pltpu
from jax.sharding import PartitionSpec as P

HEADS = 8
KVH = 2
GRID_W = 64
EPSILON = 1e-06
THETA = 10000.0
LANES = 128
MESH = pl.DeviceIdType.MESH
F32 = jnp.float32
BF16 = jnp.bfloat16


def rotary_tables(seq_total, head_dim):
    quarter = head_dim // 4
    inverse = np.float32(THETA) ** (
        -(np.float32(2.0) * np.arange(quarter, dtype=np.float32)) / np.float32(head_dim // 2)
    )
    inverse = inverse.astype(np.float32)
    rows = (np.arange(seq_total // GRID_W) - seq_total // GRID_W // 2).astype(np.float32)
    cols = (np.arange(GRID_W) - GRID_W // 2).astype(np.float32)
    sign = np.where((np.arange(head_dim) // quarter) % 2 == 0, -1.0, 1.0).astype(np.float32)

    def tables(positions):
        angle = np.tile((positions[:, None] * inverse[None, :]).astype(np.float32), (1, 4))
        angle = angle.astype(np.float64)
        return np.stack([np.cos(angle), np.sin(angle) * sign]).astype(np.float32)

    return tables(rows), tables(cols)


def ring_kernel(
    n_sp,
    n_tp,
    row_tab,
    col_tab,
    q_ref,
    k_ref,
    v_ref,
    qg_ref,
    kg_ref,
    res_ref,
    ow_ref,
    mg_ref,
    fg_ref,
    g_ref,
    u_ref,
    d_ref,
    cg_ref,
    cv_ref,
    out_ref,
    kv,
    q_rot,
    top,
    den,
    acc,
    att_own,
    att_all,
    ow_all,
    mix,
    stream,
    normed,
    wbuf,
    ups,
    partial_up,
    gated,
    hidden,
    part,
    pair_in,
    pair_sum,
    far_in,
    near_in,
    kv_s,
    kv_r,
    sib_s,
    sib_r,
    xp_s,
    xp_r,
    rel_s,
    rel_r,
    w_s,
    w_r,
    y_s,
    y_r,
    ow_s,
    ow_r,
    nm_s,
    nm_r,
    a2a_s,
    a2a_r,
    halo_s,
    halo_r,
    pair_s,
    pair_r,
    far_s,
    far_r,
    near_s,
    near_r,
):
    half = n_sp // 2
    n_x = n_tp // 2
    tok = q_ref.shape[0]
    own = res_ref.shape[0]
    model = res_ref.shape[1]
    units = g_ref.shape[0]
    common = units * 4 // 11 // 16 * 16
    private = (units - common) // 2
    kv_common = tok // 4 // 32 * 32
    kv_private = (tok - kv_common) // 2
    sources = (g_ref, u_ref, d_ref)

    g = lax.axis_index("grp")
    s = lax.axis_index("sp")
    t = lax.axis_index("tp")
    x, c = t // 2, t % 2
    z_right, z_left = (s + 1) % n_sp, (s + n_sp - 1) % n_sp
    partner = g + 1 - 2 * (g % 2)
    sibling = t + 1 - 2 * c
    x_right = 2 * ((x + 1) % n_x) + c
    x_left = 2 * ((x + n_x - 1) % n_x) + c
    kv_head = t // (HEADS // KVH)
    x_pair = x + 1 - 2 * (x % 2)
    x_cross = (x + n_x - 1 + 2 * (x % 2)) % n_x

    barrier = pltpu.get_barrier_semaphore()
    peers = [{"sp": z_right}, {"sp": z_left}, {"grp": partner}]
    peers += [{"tp": (t + i) % n_tp} for i in range(1, n_tp)]
    for peer in peers:
        pl.semaphore_signal(barrier, inc=1, device_id=peer, device_id_type=MESH)

    def remote(src, dst, send, recv, device):
        return pltpu.make_async_remote_copy(
            src_ref=src,
            dst_ref=dst,
            send_sem=send,
            recv_sem=recv,
            device_id=device,
            device_id_type=MESH,
        )

    def block_of(direction, step):
        return (s + n_sp - step) % n_sp if direction == 0 else (s + step) % n_sp

    def z_device(direction):
        return {"sp": z_right if direction == 0 else z_left}

    def kv_at(which, block, piece, side):
        if piece == 0:
            start, size = side * (kv_private + kv_common), kv_private
        else:
            start, size = kv_private, kv_common
        return kv.at[which, pl.ds(pl.multiple_of(block * tok + start, 16), size), :]

    def kv_copy(direction, step, piece, block):
        ref = kv_at(c, block, piece, x % 2)
        i = (direction * half + step) * 2 + piece
        return remote(ref, ref, kv_s.at[i], kv_r.at[i], z_device(direction))

    def sib_copy(which, direction, step, piece, block):
        ref = kv_at(which, block, piece, x % 2)
        i = (direction * half + step) * 2 + piece
        return remote(ref, ref, sib_s.at[i], sib_r.at[i], {"tp": sibling})

    def xp_copy(direction, step, block, mine):
        ref = kv_at(c, block, 0, x % 2 if mine else 1 - x % 2)
        i = direction * half + step
        return remote(ref, ref, xp_s.at[i], xp_r.at[i], {"tp": 2 * x_pair + c})

    def rel_copy(which, direction, step, block):
        ref = kv_at(which, block, 0, 1 - x % 2)
        i = direction * half + step
        return remote(ref, ref, rel_s.at[i], rel_r.at[i], {"tp": sibling})

    def w_rows(a, piece, side):
        if a == 0:
            start, size = side * (units // 2) + piece * (units // 4), units // 4
        elif piece == 0:
            start, size = side * (private + common), private
        else:
            start, size = private, common
        return pl.ds(pl.multiple_of(start, 16), size)

    def over_y(a, piece):
        return a == 0 or piece == 0

    def w_at(a, block, rows):
        return wbuf.at[a, rows, pl.ds(pl.multiple_of(block * LANES, LANES), LANES)]

    def w_copy(a, direction, step, piece, block, first=False):
        rows = w_rows(a, piece, g % 2)
        dst = w_at(a, block, rows)
        src = sources[a].at[rows, :] if first else dst
        i = ((a * 2 + direction) * half + step) * 2 + piece
        return remote(src, dst, w_s.at[i], w_r.at[i], z_device(direction))

    def y_copy(a, direction, step, piece, block, mine):
        ref = w_at(a, block, w_rows(a, piece, g % 2 if mine else 1 - g % 2))
        i = ((a * 2 + direction) * half + step) * 2 + piece
        return remote(ref, ref, y_s.at[i], y_r.at[i], {"grp": partner})

    def w_start(arrays):
        for piece in range(2):
            for a in arrays:
                for direction in range(2):
                    w_copy(a, direction, 0, piece, s, first=True).start()

    def when(condition):
        if isinstance(condition, bool):
            return (lambda f: f()) if condition else (lambda f: None)
        return pl.when(condition)

    def w_serve(arrays, k, pieces=(0, 1)):
        for piece in pieces:
            for a in arrays:
                for direction in range(2):
                    last = direction == piece
                    block = block_of(direction, k)

                    @when((k >= 1) & (k <= half if last else k < half))
                    def _():
                        w_copy(a, direction, k - 1, piece, block).wait_recv()

                        @when(k <= half - 1 if last else k <= half - 2)
                        def _():
                            w_copy(a, direction, k, piece, block).start()

                        if over_y(a, piece):
                            y_copy(a, direction, k - 1, piece, block, True).start()

    def x_gather(buf, rows, first, send, recv):
        hold = rows // 2

        def at(block, lo, size):
            return buf.at[pl.ds(pl.multiple_of(block * rows + lo, 16), size), :]

        def ring(direction, step, chip, lo, size, src=None):
            dst = at(2 * chip + c, lo, size)
            i = direction * 2 + step
            device = {"tp": x_right if direction == 0 else x_left}
            return remote(dst if src is None else src, dst, send.at[i], recv.at[i], device)

        def share(i, chip, core, lo, size, src=None):
            dst = at(2 * chip + core, lo, size)
            return remote(
                dst if src is None else src, dst, send.at[4 + i], recv.at[4 + i], {"tp": sibling}
            )

        chips = ((x + n_x - 1) % n_x, (x + 1) % n_x)
        far = (x + 2) % n_x

        def start():
            for direction in range(2):
                ring(direction, 0, x, 0, rows, first).start()
            share(4, x, c, 0, rows, first).start()

        def middle():
            for direction in range(2):
                chip = chips[direction]
                ring(direction, 0, chip, 0, rows).wait_recv()
                ring(direction, 1, chip, direction * hold, hold).start()
                share(direction, chip, c, 0, rows).start()

        def end():
            for direction in range(2):
                ring(direction, 1, far, direction * hold, hold).wait_recv()
                share(2 + direction, far, c, direction * hold, hold).start()

        def arrived():
            other = 1 - c
            share(4, x, other, 0, rows).wait_recv()
            for direction in range(2):
                share(direction, chips[direction], other, 0, rows).wait_recv()
                share(2 + direction, far, other, direction * hold, hold).wait_recv()

        def sent():
            for direction in range(2):
                ring(direction, 0, x, 0, rows, first).wait_send()
                ring(direction, 1, chips[direction], direction * hold, hold).wait_send()
                share(direction, chips[direction], c, 0, rows).wait_send()
                share(2 + direction, far, c, direction * hold, hold).wait_send()
            share(4, x, c, 0, rows, first).wait_send()

        return start, middle, end, arrived, sent

    ow_rows = ow_ref.shape[0]
    ow_parts = ow_rows // 16
    ow_far = x_cross + 1 - 2 * (x_cross % 2)

    def ow_copy(i, chip, core, lo, size, device, first=False):
        dst = ow_all.at[pl.ds(pl.multiple_of((2 * chip + core) * ow_rows + lo, 16), size), :]
        src = ow_ref.at[pl.ds(lo, size), :] if first else dst
        return remote(src, dst, ow_s.at[i], ow_r.at[i], {"tp": device})

    size = ow_rows // ow_parts

    def ow_pair(q, chip, first=False):
        return ow_copy(q, chip, c, q * size, size, 2 * x_pair + c, first)

    def ow_over(chip, first=False):
        return ow_copy(ow_parts, chip, c, 0, ow_rows, 2 * x_cross + c, first)

    def ow_on(q, chip):
        return ow_copy(ow_parts + 1 + q, chip, c, q * size, size, 2 * x_cross + c)

    def ow_own(core, first=False):
        return ow_copy(2 * ow_parts + 1, x, core, 0, ow_rows, sibling, first)

    def ow_share(i, chip, core, lo, size):
        return ow_copy(2 * ow_parts + 2 + i, chip, core, lo, size, sibling)

    def ow_shares(core, i):
        if i == ow_parts:
            return ow_share(i, x_cross, core, 0, ow_rows)
        if i < ow_parts:
            return ow_share(i, x_pair, core, i * size, size)
        return ow_share(i, ow_far, core, (i - ow_parts - 1) * size, size)

    def ow_take(q):
        ow_pair(q, x_pair).wait_recv()
        ow_on(q, x_pair).start()
        ow_shares(c, q).start()

    def ow_across():
        ow_over(x_cross).wait_recv()
        ow_shares(c, ow_parts).start()

    def ow_take_far(q):
        ow_on(q, ow_far).wait_recv()
        ow_shares(c, ow_parts + 1 + q).start()

    nm_start, nm_middle, nm_end, nm_arrived, nm_sent = x_gather(normed, own, None, nm_s, nm_r)

    grid_rows = tok // GRID_W
    lane = lax.broadcasted_iota(jnp.int32, (GRID_W, LANES), 1)
    quarter = LANES // 4

    def prepare(raw, gain, grid_row, factor):
        floats = raw.astype(F32)
        mean = jnp.sum(floats * floats, axis=-1, keepdims=True) * (1.0 / LANES)
        n = floats * lax.rsqrt(mean + EPSILON) * gain
        at = s * grid_rows + grid_row
        cos = jnp.where(lane < LANES // 2, row_tab[0, pl.ds(at, 1), :], col_tab[0])
        sin = jnp.where(lane < LANES // 2, row_tab[1, pl.ds(at, 1), :], col_tab[1])
        turned = jnp.where(
            (lane // quarter) % 2 == 0,
            pltpu.roll(n, LANES - quarter, 1),
            pltpu.roll(n, quarter, 1),
        )
        return ((n * cos + turned * sin) * factor).astype(BF16)

    head_cols = pl.ds(pl.multiple_of(kv_head * LANES, LANES), LANES)

    @pl.loop(0, grid_rows)
    def _(r):
        rows = pl.ds(pl.multiple_of(r * GRID_W, GRID_W), GRID_W)
        into = pl.ds(pl.multiple_of(s * tok + r * GRID_W, GRID_W), GRID_W)
        kv[0, into, :] = prepare(k_ref[rows, head_cols], kg_ref[...], r, 1.0)
        kv[1, into, :] = v_ref[rows, head_cols]

    pl.semaphore_wait(barrier, len(peers))
    for piece in range(2):
        for direction in range(2):
            kv_copy(direction, 0, piece, s).start()
    ow_over(x, first=True).start()
    ow_own(c, first=True).start()
    w_start((0,))

    @pl.loop(0, grid_rows)
    def _(r):
        rows = pl.ds(pl.multiple_of(r * GRID_W, GRID_W), GRID_W)
        q_rot[rows, :] = prepare(q_ref[rows, :], qg_ref[...], r, LANES ** (-0.5))

    top[...] = jnp.full_like(top, -1e30)
    den[...] = jnp.zeros_like(den)
    acc[...] = jnp.zeros_like(acc)
    for a in range(3):
        wbuf[a, :, pl.ds(pl.multiple_of(s * LANES, LANES), LANES)] = sources[a][...]
    ow_all[pl.ds(pl.multiple_of(t * ow_rows, 16), ow_rows), :] = ow_ref[...]

    chunk = min(256, tok)

    def attend(block):
        keys = pl.ds(pl.multiple_of(block * tok, tok), tok)

        @pl.loop(0, tok // chunk, unroll=True)
        def _(i):
            rows = pl.ds(pl.multiple_of(i * chunk, chunk), chunk)
            scores = lax.dot_general(
                q_rot[rows, :],
                kv[0, keys, :],
                (((1,), (1,)), ((), ())),
                preferred_element_type=F32,
            )
            before = top[rows, :]
            newest = jnp.maximum(before, jnp.max(scores, axis=1, keepdims=True))
            wide = jnp.concatenate([newest] * (tok // LANES), axis=1)
            weights = jnp.exp(scores - wide)
            fade = jnp.exp(before - newest)
            den[rows, :] = den[rows, :] * fade + jnp.sum(weights, axis=1, keepdims=True)
            acc[rows, :] = acc[rows, :] * fade + jnp.dot(
                weights.astype(BF16), kv[1, keys, :], preferred_element_type=F32
            )
            top[rows, :] = newest

    ow_in_loop = min(ow_parts, max(half - 4, 0))
    @pl.loop(1, half + 3)
    def _(k):
        def at_step(step, act):
            @pl.when(k == min(step, half + 2))
            def _():
                act()

        def kv_serve(piece):
            for direction in range(2):
                last = direction == piece
                block = block_of(direction, k)

                @pl.when(k <= half if last else k < half)
                def _():
                    kv_copy(direction, k - 1, piece, block).wait_recv()

                    @pl.when(k <= half - 1 if last else k <= half - 2)
                    def _():
                        kv_copy(direction, k, piece, block).start()

                    if piece == 0:
                        xp_copy(direction, k - 1, block, True).start()
                    sib_copy(c, direction, k - 1, piece, block).start()

        kv_serve(0)
        for q in range(ow_parts):
            at_step(1 + q, lambda: ow_pair(q, x, first=True).start())
        w_serve((0,), k - 1, (0,))
        for direction in range(2):
            block = block_of(direction, k - 1)

            @pl.when((k >= 2) & (k <= half + 1 if direction == 0 else k <= half))
            def _():
                xp_copy(direction, k - 2, block, False).wait_recv()
                rel_copy(c, direction, k - 2, block).start()

        for direction in range(2):
            block = block_of(direction, k - 2)
            for piece in range(2):
                last = direction == piece

                @pl.when((k >= 3) & (k <= half + 2 if last else k <= half + 1))
                def _():
                    sib_copy(1 - c, direction, k - 3, piece, block).wait_recv()

            @pl.when((k >= 3) & (k <= half + 2 if direction == 0 else k <= half + 1))
            def _():
                rel_copy(1 - c, direction, k - 3, block).wait_recv()

        @pl.when(k != 2)
        def _():
            attend((s + n_sp - jnp.where(k == 1, 0, k - 2)) % n_sp)

        kv_serve(1)
        w_serve((0,), k - 1, (1,))
        for q in range(ow_parts):
            at_step(3 + q, lambda: ow_take(q))
        at_step(5, ow_across)
        for q in range(ow_in_loop):
            at_step(6 + q, lambda: ow_take_far(q))
        at_step(half, lambda: w_start((1,)))

        @pl.when((k >= 3) & (k <= half + 1))
        def _():
            attend((s + k - 2) % n_sp)

        at_step(half + 2, lambda: w_serve((1,), 1))

    def vd_serve(k):
        for piece in range(2):
            w_serve((1,), k, (piece,))
            w_serve((2,), k - 2, (piece,))
        if k == 2:
            w_start((2,))

    att_own[...] = (acc[...] / den[...]).astype(BF16)

    def att_copy(i, to, source):
        cols = pl.ds(pl.multiple_of(source * LANES, LANES), LANES)
        rows = pl.ds(pl.multiple_of(to * own, 16), own)
        return remote(
            att_own.at[rows, :],
            att_all.at[:, cols],
            a2a_s.at[i - 1],
            a2a_r.at[i - 1],
            {"tp": to},
        )

    for i in range(1, n_tp):
        att_copy(i, (t + i) % n_tp, t).start()
    att_all[:, pl.ds(pl.multiple_of(t * LANES, LANES), LANES)] = att_own[
        pl.ds(pl.multiple_of(t * own, 16), own), :
    ]
    vd_serve(2)
    for q in range(ow_in_loop, ow_parts):
        ow_take_far(q)
    for i in range(2 * ow_parts + 1):
        ow_shares(1 - c, i).wait_recv()
    ow_own(1 - c).wait_recv()
    for i in range(1, n_tp):
        att_copy(i, t, (t + n_tp - i) % n_tp).wait_recv()

    width = min(512, model)

    @pl.loop(0, model // width)
    def _(j):
        cols = pl.ds(pl.multiple_of(j * width, width), width)
        total = jnp.zeros((own, width), F32)
        for head in range(n_tp):
            span = slice(head * LANES, (head + 1) * LANES)
            total += (
                jnp.dot(att_all[:, span], ow_all[span, cols], preferred_element_type=F32)
                .astype(BF16)
                .astype(F32)
            )
        mix[:, cols] = total

    @pl.loop(0, own // 16)
    def _(r):
        rows = pl.ds(pl.multiple_of(r * 16, 16), 16)
        m = mix[rows, :]
        scale = lax.rsqrt(jnp.mean(m * m, axis=-1, keepdims=True) + EPSILON)
        added = (res_ref[rows, :].astype(F32) + m * scale * mg_ref[...]).astype(BF16)
        stream[rows, :] = added
        f = added.astype(F32)
        scale = lax.rsqrt(jnp.mean(f * f, axis=-1, keepdims=True) + EPSILON)
        normed[pl.ds(pl.multiple_of(t * own + r * 16, 16), 16), :] = (
            f * scale * fg_ref[...]
        ).astype(BF16)

    vd_serve(3)
    nm_start()
    vd_serve(4)
    vd_serve(5)
    nm_middle()
    vd_serve(6)
    nm_end()
    vd_serve(7)
    nm_arrived()

    def y_arrived(a, step):
        for direction in range(2):
            for piece in range(2):

                @when((step < half - 1) | (direction == piece))
                def _():
                    if over_y(a, piece):
                        block = block_of(direction, step + 1)
                        y_copy(a, direction, step, piece, block, False).wait_recv()

    def halo_copy(direction):
        src = normed.at[pl.ds(tok - 8 if direction == 0 else 0, 8), :]
        dst = normed.at[pl.ds(tok + 8 * direction, 8), :]
        return remote(src, dst, halo_s.at[direction], halo_r.at[direction], z_device(direction))

    for direction in range(2):
        halo_copy(direction).start()
    if half >= 8:
        vd_serve(half)
    for step in range(half):
        y_arrived(0, step)
    for direction in range(2):
        halo_copy(direction).wait_recv()

    m_rows = min(256, tok)
    m_count = tok // m_rows

    def put_up(a, made, i):
        made = made.astype(BF16).astype(F32)
        ups[a, pl.ds(8 + i * m_rows, m_rows), :] = made[:m_rows]
        if i == m_count - 1:
            ups[a, pl.ds(0, 8), :] = jnp.where(s == 0, 0.0, made[m_rows : m_rows + 8])
            ups[a, pl.ds(tok + 8, 8), :] = jnp.where(s == n_sp - 1, 0.0, made[m_rows + 8 :])

    def up_rows(i):
        return pl.ds(i * m_rows, m_rows + (16 if i == m_count - 1 else 0))

    for i in range(m_count):
        made = lax.dot_general(
            normed[up_rows(i), :],
            wbuf[0],
            (((1,), (1,)), ((), ())),
            preferred_element_type=F32,
        )
        put_up(0, made, i)

    done = half - 2 if half >= 8 else half
    w_serve((2,), done + 1)

    c_rows = min(32, own)

    def by_core(row):
        to = row // own
        start = ((to % 2) * n_x + to // 2) * own + row % own
        return pl.ds(pl.multiple_of(start, c_rows), c_rows)

    def convolved(a, taps, row):
        near = ups[a, pl.ds(pl.multiple_of(row, c_rows), c_rows + 16), :]
        return (
            taps[0:1, :] * near[7 : 7 + c_rows]
            + taps[1:2, :] * near[8 : 8 + c_rows]
            + taps[2:3, :] * near[9 : 9 + c_rows]
        )

    def blocks(j):
        return (s + n_sp - j) % n_sp, (s + j % half) % n_sp

    def cols(block):
        return pl.ds(pl.multiple_of(block * LANES, LANES), LANES)

    def up_value(j, fresh=False, last=False):
        pair = blocks(j)
        weights = jnp.concatenate([wbuf[1, :, cols(b)] for b in pair], axis=1)
        for i in range(m_count):
            tokens = jnp.concatenate([normed[up_rows(i), cols(b)] for b in pair], axis=1)
            made = lax.dot_general(
                tokens, weights, (((1,), (1,)), ((), ())), preferred_element_type=F32
            )
            if not fresh:
                made += partial_up[up_rows(i), :]
            if last:
                put_up(1, made, i)
            else:
                partial_up[up_rows(i), :] = made

    if half > 1:
        y_arrived(1, 0)
        up_value(1, fresh=True)

        @pl.loop(2, half)
        def _(j):
            y_arrived(1, j - 1)
            up_value(j)

    w_serve((2,), done + 2)
    y_arrived(1, half - 1)
    up_value(half, last=True)
    done += 2

    @pl.loop(0, tok // c_rows)
    def _(i):
        row = i * c_rows
        v = convolved(0, cg_ref, row)
        inner = (2.0 / np.pi) ** 0.5 * (v + 0.044715 * (v * v * v))
        gated[pl.ds(pl.multiple_of(row, c_rows), c_rows), :] = 0.5 * v * (1.0 + jnp.tanh(inner))

    @pl.loop(0, tok // c_rows)
    def _(i):
        row = i * c_rows
        gate = gated[pl.ds(pl.multiple_of(row, c_rows), c_rows), :]
        hidden[by_core(row), :] = (gate * convolved(1, cv_ref, row)).astype(BF16)

    per_core = n_x * own
    cut = own // 2
    chip_right, chip_left = (x + 1) % n_x, (x + n_x - 1) % n_x
    chip_far = (x + 2) % n_x

    def pair_copy(i, block, core):
        rows = pl.ds(pl.multiple_of(core * per_core, 16), per_core)
        return remote(
            part.at[block, rows, :],
            pair_in.at[block],
            pair_s.at[i],
            pair_r.at[i],
            {"tp": sibling},
        )

    def far_copy(direction, block):
        lo = cut if direction == 0 else 0
        return remote(
            pair_sum.at[block, pl.ds(pl.multiple_of(chip_far * own + lo, 16), cut), :],
            far_in.at[direction, block],
            far_s.at[direction * n_sp + block],
            far_r.at[direction * n_sp + block],
            {"tp": x_right if direction == 0 else x_left},
        )

    def near_copy(direction, block):
        chip = chip_right if direction == 0 else chip_left
        return remote(
            pair_sum.at[block, pl.ds(pl.multiple_of(chip * own, 16), own), :],
            near_in.at[direction, block],
            near_s.at[direction],
            near_r.at[direction],
            {"tp": x_right if direction == 0 else x_left},
        )

    def near_all(direction):
        ref = near_in.at[direction]
        return remote(
            ref,
            ref,
            near_s.at[direction],
            near_r.at[direction],
            {"tp": x_right if direction == 0 else x_left},
        )

    def of_core(chip, size, lo=0):
        return pl.ds(pl.multiple_of(c * per_core + chip * own + lo, 16), size)

    def of_chip(chip, size, lo=0):
        return pl.ds(pl.multiple_of(chip * own + lo, 16), size)

    sum_lag, send_lag = 2, 4

    @pl.loop(1, half + send_lag + 1)
    def _(j):
        @pl.when(j <= half)
        def _():
            @pl.when(j > done)
            def _():
                w_serve((2,), j)

            y_arrived(2, j - 1)
            first, second = blocks(j)

            @pl.loop(0, m_count)
            def _(i):
                rows = pl.ds(pl.multiple_of(i * m_rows, m_rows), m_rows)
                both = jnp.concatenate([wbuf[2, :, cols(first)], wbuf[2, :, cols(second)]], axis=1)
                made = jnp.dot(hidden[rows, :], both, preferred_element_type=F32).astype(BF16)
                part[first, rows, :] = made[:, :LANES]
                part[second, rows, :] = made[:, LANES:]


            for i, block in enumerate((first, second)):
                pair_copy(2 * (j - 1) + i, block, 1 - c).start()

        @pl.when((j > sum_lag) & (j <= half + sum_lag))
        def _():
            for i, block in enumerate(blocks(j - sum_lag)):
                pair_copy(2 * (j - sum_lag - 1) + i, block, c).wait_recv()
                for chip in (chip_far, chip_right, chip_left):
                    pair_sum[block, of_chip(chip, own), :] = (
                        part[block, of_core(chip, own), :].astype(F32)
                        + pair_in[block, of_chip(chip, own), :].astype(F32)
                    ).astype(BF16)
                for direction in range(2):
                    far_copy(direction, block).start()

        @pl.when(j > send_lag)
        def _():
            for block in blocks(j - send_lag):
                for direction in range(2):
                    far_copy(direction, block).wait_recv()
                    chip = chip_right if direction == 0 else chip_left
                    lo = cut if direction == 0 else 0
                    pair_sum[block, of_chip(chip, cut, lo), :] = (
                        part[block, of_core(chip, cut, lo), :].astype(F32)
                        + pair_in[block, of_chip(chip, cut, lo), :].astype(F32)
                        + far_in[direction, block].astype(F32)
                    ).astype(BF16)
                    near_copy(direction, block).start()

    for direction in range(2):
        near_all(direction).wait_recv()

    for b in range(n_sp):
        span = slice(b * LANES, (b + 1) * LANES)
        total = part[b, of_core(x, own), :].astype(F32) + pair_in[b, of_chip(x, own), :].astype(F32)
        for direction in range(2):
            total += near_in[direction, b].astype(F32)
        out_ref[:, span] = (stream[:, span].astype(F32) + total).astype(BF16)

    for q in range(ow_parts):
        ow_pair(q, x, first=True).wait_send()
        ow_on(q, x_pair).wait_send()
    ow_over(x, first=True).wait_send()
    for i in range(2 * ow_parts + 1):
        ow_shares(c, i).wait_send()
    ow_own(c, first=True).wait_send()
    nm_sent()
    for i in range(1, n_tp):
        att_copy(i, (t + i) % n_tp, t).wait_send()
    for b in range(n_sp):
        pair_copy(b, b, 1 - c).wait_send()
        for direction in range(2):
            far_copy(direction, b).wait_send()
    for direction in range(2):
        near_all(direction).wait_send()
        halo_copy(direction).wait_send()
        for step in range(half):
            for piece in range(2):
                if step == half - 1 and direction != piece:
                    continue
                block = block_of(direction, step)
                kv_copy(direction, step, piece, block).wait_send()
                sib_copy(c, direction, step, piece, block_of(direction, step + 1)).wait_send()
                arriving = block_of(direction, step + 1)
                if piece == 0:
                    xp_copy(direction, step, arriving, True).wait_send()
                    rel_copy(c, direction, step, arriving).wait_send()
                for a in range(3):
                    w_copy(a, direction, step, piece, block, first=step == 0).wait_send()
                    if over_y(a, piece):
                        y_copy(a, direction, step, piece, arriving, True).wait_send()


def body(
    queries,
    keys,
    values,
    query_gain,
    key_gain,
    residual,
    out_weight,
    mix_gain,
    ffn_gain,
    gate_in,
    value_in,
    conv_gate,
    conv_value,
    down_t,
):
    n_sp, n_tp = lax.axis_size("sp"), lax.axis_size("tp")
    half = n_sp // 2
    tok = queries.shape[0]
    own, model = residual.shape
    units = gate_in.shape[1]
    row_tab, col_tab = rotary_tables(tok * n_sp, query_gain.shape[0])
    vmem = pl.BlockSpec(memory_space=pltpu.VMEM)
    dma = pltpu.SemaphoreType.DMA
    operands = (
        jnp.asarray(row_tab),
        jnp.asarray(col_tab),
        queries,
        keys,
        values,
        query_gain[None, :],
        key_gain[None, :],
        residual,
        out_weight,
        mix_gain[None, :],
        ffn_gain[None, :],
        gate_in.T,
        value_in.T,
        down_t.T,
        conv_gate,
        conv_value,
    )
    return pl.pallas_call(
        functools.partial(ring_kernel, n_sp, n_tp),
        out_shape=jax.ShapeDtypeStruct((own, model), BF16),
        in_specs=[vmem] * len(operands),
        out_specs=vmem,
        scratch_shapes=[
            pltpu.VMEM((2, tok * n_sp, LANES), BF16),
            pltpu.VMEM((tok, LANES), BF16),
            pltpu.VMEM((tok, LANES), F32),
            pltpu.VMEM((tok, LANES), F32),
            pltpu.VMEM((tok, LANES), F32),
            pltpu.VMEM((tok, LANES), BF16),
            pltpu.VMEM((own, n_tp * LANES), BF16),
            pltpu.VMEM((n_tp * out_weight.shape[0], model), BF16),
            pltpu.VMEM((own, model), F32),
            pltpu.VMEM((own, model), BF16),
            pltpu.VMEM((tok + 16, model), BF16),
            pltpu.VMEM((3, units, model), BF16),
            pltpu.VMEM((2, tok + 16, units), F32),
            pltpu.VMEM((tok + 16, units), F32),
            pltpu.VMEM((tok, units), F32),
            pltpu.VMEM((tok, units), BF16),
            pltpu.VMEM((n_sp, tok, LANES), BF16),
            pltpu.VMEM((n_sp, tok // 2, LANES), BF16),
            pltpu.VMEM((n_sp, tok // 2, LANES), BF16),
            pltpu.VMEM((2, n_sp, own // 2, LANES), BF16),
            pltpu.VMEM((2, n_sp, own, LANES), BF16),
            dma((4 * half,)),
            dma((4 * half,)),
            dma((4 * half,)),
            dma((4 * half,)),
            dma((2 * half,)),
            dma((2 * half,)),
            dma((2 * half,)),
            dma((2 * half,)),
            dma((12 * half,)),
            dma((12 * half,)),
            dma((12 * half,)),
            dma((12 * half,)),
            dma((4 * (out_weight.shape[0] // 16) + 3,)),
            dma((4 * (out_weight.shape[0] // 16) + 3,)),
            dma((9,)),
            dma((9,)),
            dma((n_tp - 1,)),
            dma((n_tp - 1,)),
            dma((2,)),
            dma((2,)),
            dma((n_sp,)),
            dma((n_sp,)),
            dma((2 * n_sp,)),
            dma((2 * n_sp,)),
            dma((2,)),
            dma((2,)),
        ],
        compiler_params=pltpu.CompilerParams(
            collective_id=0,
            has_side_effects=True,
            vmem_limit_bytes=62 * 1024 * 1024,
        ),
        name="layer",
    )(*operands)


def solution(mesh):
    return jax.shard_map(
        body,
        mesh=mesh,
        in_specs=(
            P(("grp", "sp"), "tp"),
            P(("grp", "sp"), None),
            P(("grp", "sp"), None),
            P(),
            P(),
            P(("grp", "sp", "tp"), None),
            P("tp", None),
            P(),
            P(),
            P("sp", "tp"),
            P("sp", "tp"),
            P(None, "tp"),
            P(None, "tp"),
            P("sp", "tp"),
        ),
        out_specs=P(("grp", "sp", "tp"), None),
        check_vma=False,
    )
```

```python
import functools

import jax
import jax.numpy as jnp
import numpy as np
from jax import lax
from jax.experimental import pallas as pl
from jax.experimental.pallas import tpu as pltpu
from jax.sharding import PartitionSpec as P

HEADS = 8
KVH = 2
GRID_W = 64
EPSILON = 1e-06
THETA = 10000.0
LANES = 128
MESH = pl.DeviceIdType.MESH
F32 = jnp.float32
BF16 = jnp.bfloat16


def rotary_tables(seq_total, head_dim):
    quarter = head_dim // 4
    inverse = np.float32(THETA) ** (
        -(np.float32(2.0) * np.arange(quarter, dtype=np.float32)) / np.float32(head_dim // 2)
    )
    inverse = inverse.astype(np.float32)
    rows = (np.arange(seq_total // GRID_W) - seq_total // GRID_W // 2).astype(np.float32)
    cols = (np.arange(GRID_W) - GRID_W // 2).astype(np.float32)
    sign = np.where((np.arange(head_dim) // quarter) % 2 == 0, -1.0, 1.0).astype(np.float32)

    def tables(positions):
        angle = np.tile((positions[:, None] * inverse[None, :]).astype(np.float32), (1, 4))
        angle = angle.astype(np.float64)
        return np.stack([np.cos(angle), np.sin(angle) * sign]).astype(np.float32)

    return tables(rows), tables(cols)


def ring_kernel(
    n_sp,
    n_tp,
    row_tab,
    col_tab,
    q_ref,
    k_ref,
    v_ref,
    qg_ref,
    kg_ref,
    res_ref,
    ow_ref,
    mg_ref,
    fg_ref,
    g_ref,
    u_ref,
    d_ref,
    cg_ref,
    cv_ref,
    out_ref,
    kv,
    q_rot,
    top,
    den,
    acc,
    att_own,
    att_all,
    ow_all,
    mix,
    stream,
    normed,
    wbuf,
    ups,
    partial_up,
    hidden,
    part,
    pair_in,
    pair_sum,
    far_in,
    near_in,
    kv_s,
    kv_r,
    sib_s,
    sib_r,
    xp_s,
    xp_r,
    w_s,
    w_r,
    y_s,
    y_r,
    ow_s,
    ow_r,
    nm_s,
    nm_r,
    a2a_s,
    a2a_r,
    halo_s,
    halo_r,
    pair_s,
    pair_r,
    far_s,
    far_r,
    near_s,
    near_r,
):
    half = n_sp // 2
    n_x = n_tp // 2
    tok = q_ref.shape[0]
    own = res_ref.shape[0]
    model = res_ref.shape[1]
    units = g_ref.shape[0]
    common = units * 4 // 11 // 16 * 16
    private = (units - common) // 2
    kv_common = tok // 4 // 32 * 32
    kv_private = (tok - kv_common) // 2
    sources = (g_ref, u_ref, d_ref)

    g = lax.axis_index("grp")
    s = lax.axis_index("sp")
    t = lax.axis_index("tp")
    x, c = t // 2, t % 2
    z_right, z_left = (s + 1) % n_sp, (s + n_sp - 1) % n_sp
    partner = g + 1 - 2 * (g % 2)
    sibling = t + 1 - 2 * c
    x_right = 2 * ((x + 1) % n_x) + c
    x_left = 2 * ((x + n_x - 1) % n_x) + c
    kv_head = t // (HEADS // KVH)
    x_pair = x + 1 - 2 * (x % 2)
    x_cross = (x + n_x - 1 + 2 * (x % 2)) % n_x

    barrier = pltpu.get_barrier_semaphore()
    peers = [{"sp": z_right}, {"sp": z_left}, {"grp": partner}]
    peers += [{"tp": (t + i) % n_tp} for i in range(1, n_tp)]
    for peer in peers:
        pl.semaphore_signal(barrier, inc=1, device_id=peer, device_id_type=MESH)

    def remote(src, dst, send, recv, device):
        return pltpu.make_async_remote_copy(
            src_ref=src,
            dst_ref=dst,
            send_sem=send,
            recv_sem=recv,
            device_id=device,
            device_id_type=MESH,
        )

    def block_of(direction, step):
        return (s + n_sp - step) % n_sp if direction == 0 else (s + step) % n_sp

    def z_device(direction):
        return {"sp": z_right if direction == 0 else z_left}

    def kv_at(which, block, piece, side):
        if piece == 0:
            start, size = side * (kv_private + kv_common), kv_private
        else:
            start, size = kv_private, kv_common
        return kv.at[which, pl.ds(pl.multiple_of(block * tok + start, 16), size), :]

    def kv_copy(direction, step, piece, block):
        ref = kv_at(c, block, piece, x % 2)
        i = (direction * half + step) * 2 + piece
        return remote(ref, ref, kv_s, kv_r.at[i], z_device(direction))

    def sib_copy(which, direction, step, piece, block):
        ref = kv_at(which, block, piece, x % 2)
        i = jnp.where(step == half - 1, 0, direction) * half + step
        return remote(ref, ref, sib_s, sib_r.at[i], {"tp": sibling})

    def xp_copy(direction, step, block, mine):
        ref = kv_at(c, block, 0, x % 2 if mine else 1 - x % 2)
        i = direction * half + step
        return remote(ref, ref, xp_s, xp_r.at[i], {"tp": 2 * x_pair + c})

    def rel_copy(which, direction, step, block):
        ref = kv_at(which, block, 0, 1 - x % 2)
        i = direction * half + step
        return remote(ref, ref, sib_s, sib_r.at[i], {"tp": sibling})

    def sib_block(which, direction, step, block):
        ref = kv.at[which, pl.ds(pl.multiple_of(block * tok, tok), tok), :]
        i = direction * half + step
        return remote(ref, ref, sib_s, sib_r.at[i], {"tp": sibling})

    def w_rows(a, piece, side):
        if a == 0:
            start, size = side * (units // 2) + piece * (units // 4), units // 4
        elif piece == 0:
            start, size = side * (private + common), private
        else:
            start, size = private, common
        return pl.ds(pl.multiple_of(start, 16), size)

    def over_y(a, piece):
        return a == 0 or piece == 0

    def w_at(a, block, rows):
        return wbuf.at[a, rows, pl.ds(pl.multiple_of(block * LANES, LANES), LANES)]

    def w_copy(a, direction, step, piece, block, first=False):
        rows = w_rows(a, piece, g % 2)
        dst = w_at(a, block, rows)
        src = sources[a].at[rows, :] if first else dst
        i = ((a * 2 + direction) * half + step) * 2 + piece
        return remote(src, dst, w_s.at[a], w_r.at[i], z_device(direction))

    def y_copy(a, direction, step, piece, block, mine):
        ref = w_at(a, block, w_rows(a, piece, g % 2 if mine else 1 - g % 2))
        i = 0 if a == 0 else 1 + (a - 1) * half + step
        return remote(ref, ref, y_s.at[a], y_r.at[i], {"grp": partner})

    def w_start(arrays):
        for piece in range(2):
            for a in arrays:
                for direction in range(2):
                    w_copy(a, direction, 0, piece, s, first=True).start()

    def when(condition):
        if isinstance(condition, bool):
            return (lambda f: f()) if condition else (lambda f: None)
        return pl.when(condition)

    def w_serve(arrays, k, pieces=(0, 1)):
        for piece in pieces:
            for a in arrays:
                for direction in range(2):
                    last = direction == piece
                    block = block_of(direction, k)

                    @when((k >= 1) & (k <= half if last else k < half))
                    def _():
                        w_copy(a, direction, k - 1, piece, block).wait_recv()

                        @when(k <= half - 1 if last else k <= half - 2)
                        def _():
                            w_copy(a, direction, k, piece, block).start()

                        if over_y(a, piece):
                            y_copy(a, direction, k - 1, piece, block, True).start()

    def x_gather(buf, rows, first, send, recv):
        hold = rows // 2

        def at(block, lo, size):
            return buf.at[pl.ds(pl.multiple_of(block * rows + lo, 16), size), :]

        def ring(direction, step, chip, lo, size, src=None):
            dst = at(2 * chip + c, lo, size)
            i = direction * 2 + step
            device = {"tp": x_right if direction == 0 else x_left}
            return remote(dst if src is None else src, dst, send, recv.at[i], device)

        def share(chip, core, lo, size, src=None):
            dst = at(2 * chip + core, lo, size)
            return remote(
                dst if src is None else src, dst, send, recv.at[4], {"tp": sibling}
            )

        chips = ((x + n_x - 1) % n_x, (x + 1) % n_x)
        far = (x + 2) % n_x

        def start():
            for direction in range(2):
                ring(direction, 0, x, 0, rows, first).start()
            share(x, c, 0, rows, first).start()

        def middle():
            for direction in range(2):
                chip = chips[direction]
                ring(direction, 0, chip, 0, rows).wait_recv()
                ring(direction, 1, chip, direction * hold, hold).start()
                share(chip, c, 0, rows).start()

        def end():
            for direction in range(2):
                ring(direction, 1, far, direction * hold, hold).wait_recv()
                share(far, c, direction * hold, hold).start()

        def all_rows(blocks):
            ref = buf.at[pl.ds(0, blocks * rows), :]
            return remote(ref, ref, send, recv.at[4], {"tp": sibling})

        def arrived():
            all_rows(n_x).wait_recv()

        def sent():
            all_rows(2 * n_x - 1).wait_send()

        return start, middle, end, arrived, sent

    ow_rows = ow_ref.shape[0]
    ow_parts = ow_rows // 16
    ow_far = x_cross + 1 - 2 * (x_cross % 2)

    def ow_copy(i, chip, core, lo, size, device, first=False):
        dst = ow_all.at[pl.ds(pl.multiple_of((2 * chip + core) * ow_rows + lo, 16), size), :]
        src = ow_ref.at[pl.ds(lo, size), :] if first else dst
        return remote(src, dst, ow_s, ow_r.at[i], {"tp": device})

    size = ow_rows // ow_parts

    def ow_pair(q, chip, first=False):
        return ow_copy(q, chip, c, q * size, size, 2 * x_pair + c, first)

    def ow_over(chip, first=False):
        return ow_copy(ow_parts, chip, c, 0, ow_rows, 2 * x_cross + c, first)

    def ow_on(q, chip):
        return ow_copy(ow_parts + 1 + q, chip, c, q * size, size, 2 * x_cross + c)

    def ow_own(core, first=False):
        return ow_copy(2 * ow_parts + 1, x, core, 0, ow_rows, sibling, first)

    def ow_share(i, chip, core, lo, size):
        return ow_copy(2 * ow_parts + 1, chip, core, lo, size, sibling)

    def ow_shares(core, i):
        if i == ow_parts:
            return ow_share(i, x_cross, core, 0, ow_rows)
        if i < ow_parts:
            return ow_share(i, x_pair, core, i * size, size)
        return ow_share(i, ow_far, core, (i - ow_parts - 1) * size, size)

    def ow_bytes(blocks):
        ref = ow_all.at[pl.ds(0, blocks * ow_rows), :]
        return remote(ref, ref, ow_s, ow_r.at[2 * ow_parts + 1], {"tp": sibling})

    def ow_take(q):
        ow_pair(q, x_pair).wait_recv()
        ow_on(q, x_pair).start()
        ow_shares(c, q).start()

    def ow_across():
        ow_over(x_cross).wait_recv()
        ow_shares(c, ow_parts).start()

    def ow_take_far(q):
        ow_on(q, ow_far).wait_recv()
        ow_shares(c, ow_parts + 1 + q).start()

    nm_start, nm_middle, nm_end, nm_arrived, nm_sent = x_gather(normed, own, None, nm_s, nm_r)

    grid_rows = tok // GRID_W
    lane = lax.broadcasted_iota(jnp.int32, (GRID_W, LANES), 1)
    quarter = LANES // 4

    def prepare(raw, gain, grid_row, factor):
        floats = raw.astype(F32)
        mean = jnp.sum(floats * floats, axis=-1, keepdims=True) * (1.0 / LANES)
        n = floats * lax.rsqrt(mean + EPSILON) * gain
        at = s * grid_rows + grid_row
        cos = jnp.where(lane < LANES // 2, row_tab[0, pl.ds(at, 1), :], col_tab[0])
        sin = jnp.where(lane < LANES // 2, row_tab[1, pl.ds(at, 1), :], col_tab[1])
        turned = jnp.where(
            (lane // quarter) % 2 == 0,
            pltpu.roll(n, LANES - quarter, 1),
            pltpu.roll(n, quarter, 1),
        )
        return ((n * cos + turned * sin) * factor).astype(BF16)

    head_cols = pl.ds(pl.multiple_of(kv_head * LANES, LANES), LANES)

    @pl.loop(0, grid_rows)
    def _(r):
        rows = pl.ds(pl.multiple_of(r * GRID_W, GRID_W), GRID_W)
        into = pl.ds(pl.multiple_of(s * tok + r * GRID_W, GRID_W), GRID_W)
        kv[0, into, :] = prepare(k_ref[rows, head_cols], kg_ref[...], r, 1.0)
        kv[1, into, :] = v_ref[rows, head_cols]

    pl.semaphore_wait(barrier, len(peers))
    for piece in range(2):
        for direction in range(2):
            kv_copy(direction, 0, piece, s).start()
    ow_over(x, first=True).start()
    ow_own(c, first=True).start()
    w_start((0,))

    @pl.loop(0, grid_rows)
    def _(r):
        rows = pl.ds(pl.multiple_of(r * GRID_W, GRID_W), GRID_W)
        q_rot[rows, :] = prepare(q_ref[rows, :], qg_ref[...], r, LANES ** (-0.5))

    top[...] = jnp.full_like(top, -1e30)
    den[...] = jnp.zeros_like(den)
    acc[...] = jnp.zeros_like(acc)
    for a in range(3):
        wbuf[a, :, pl.ds(pl.multiple_of(s * LANES, LANES), LANES)] = sources[a][...]
    ow_all[pl.ds(pl.multiple_of(t * ow_rows, 16), ow_rows), :] = ow_ref[...]

    chunk = min(256, tok)

    def attend(block):
        keys = pl.ds(pl.multiple_of(block * tok, tok), tok)

        @pl.loop(0, tok // chunk, unroll=True)
        def _(i):
            rows = pl.ds(pl.multiple_of(i * chunk, chunk), chunk)
            scores = lax.dot_general(
                q_rot[rows, :],
                kv[0, keys, :],
                (((1,), (1,)), ((), ())),
                preferred_element_type=F32,
            )
            before = top[rows, :]
            newest = jnp.maximum(before, jnp.max(scores, axis=1, keepdims=True))
            wide = jnp.concatenate([newest] * (tok // LANES), axis=1)
            weights = jnp.exp(scores - wide)
            fade = jnp.exp(before - newest)
            den[rows, :] = den[rows, :] * fade + jnp.sum(weights, axis=1, keepdims=True)
            acc[rows, :] = acc[rows, :] * fade + jnp.dot(
                weights.astype(BF16), kv[1, keys, :], preferred_element_type=F32
            )
            top[rows, :] = newest

    ow_in_loop = min(ow_parts, max(half - 4, 0))
    @pl.loop(1, half + 3)
    def _(k):
        def at_step(step, act):
            @pl.when(k == min(step, half + 2))
            def _():
                act()

        def kv_serve(piece):
            for direction in range(2):
                last = direction == piece
                block = block_of(direction, k)

                @pl.when(k <= half if last else k < half)
                def _():
                    kv_copy(direction, k - 1, piece, block).wait_recv()

                    @pl.when(k <= half - 1 if last else k <= half - 2)
                    def _():
                        kv_copy(direction, k, piece, block).start()

                    if piece == 0:
                        xp_copy(direction, k - 1, block, True).start()
                    sib_copy(c, direction, k - 1, piece, block).start()

        kv_serve(0)
        for q in range(ow_parts):
            at_step(1 + q, lambda: ow_pair(q, x, first=True).start())
        w_serve((0,), k - 1, (0,))
        for direction in range(2):
            block = block_of(direction, k - 1)

            @pl.when((k >= 2) & (k <= half + 1 if direction == 0 else k <= half))
            def _():
                xp_copy(direction, k - 2, block, False).wait_recv()
                rel_copy(c, direction, k - 2, block).start()

        for direction in range(2):
            block = block_of(direction, k - 2)

            @pl.when((k >= 3) & (k <= half + 2 if direction == 0 else k <= half + 1))
            def _():
                sib_block(1 - c, direction, k - 3, block).wait_recv()

        @pl.when(k != 2)
        def _():
            attend((s + n_sp - jnp.where(k == 1, 0, k - 2)) % n_sp)

        kv_serve(1)
        w_serve((0,), k - 1, (1,))
        for q in range(ow_parts):
            at_step(3 + q, lambda: ow_take(q))
        at_step(5, ow_across)
        for q in range(ow_in_loop):
            at_step(6 + q, lambda: ow_take_far(q))
        at_step(half, lambda: w_start((1,)))

        @pl.when((k >= 3) & (k <= half + 1))
        def _():
            attend((s + k - 2) % n_sp)

        at_step(half + 2, lambda: w_serve((1,), 1))

    d_lag = 2

    def vd_serve(k):
        for piece in range(2):
            w_serve((1,), k, (piece,))
            w_serve((2,), k - d_lag, (piece,))
        if k == d_lag:
            w_start((2,))

    att_own[...] = (acc[...] / den[...]).astype(BF16)

    def att_copy(to, source):
        cols = pl.ds(pl.multiple_of(source * LANES, LANES), LANES)
        rows = pl.ds(pl.multiple_of(to * own, 16), own)
        return remote(
            att_own.at[rows, :],
            att_all.at[:, cols],
            a2a_s,
            a2a_r,
            {"tp": to},
        )

    for i in range(1, n_tp):
        att_copy((t + i) % n_tp, t).start()
    att_all[:, pl.ds(pl.multiple_of(t * LANES, LANES), LANES)] = att_own[
        pl.ds(pl.multiple_of(t * own, 16), own), :
    ]
    vd_serve(2)
    for q in range(ow_in_loop, ow_parts):
        ow_take_far(q)
    ow_bytes(n_x).wait_recv()
    def att_bytes():
        ref = att_all.at[:, pl.ds(0, (n_tp - 1) * LANES)]
        return remote(ref, ref, a2a_s, a2a_r, {"tp": sibling})

    att_bytes().wait_recv()

    width = min(512, model)

    @pl.loop(0, model // width)
    def _(j):
        cols = pl.ds(pl.multiple_of(j * width, width), width)
        total = jnp.zeros((own, width), F32)
        for head in range(n_tp):
            span = slice(head * LANES, (head + 1) * LANES)
            total += (
                jnp.dot(att_all[:, span], ow_all[span, cols], preferred_element_type=F32)
                .astype(BF16)
                .astype(F32)
            )
        mix[:, cols] = total

    @pl.loop(0, own // 16)
    def _(r):
        rows = pl.ds(pl.multiple_of(r * 16, 16), 16)
        m = mix[rows, :]
        scale = lax.rsqrt(jnp.mean(m * m, axis=-1, keepdims=True) + EPSILON)
        added = (res_ref[rows, :].astype(F32) + m * scale * mg_ref[...]).astype(BF16)
        stream[rows, :] = added
        f = added.astype(F32)
        scale = lax.rsqrt(jnp.mean(f * f, axis=-1, keepdims=True) + EPSILON)
        normed[pl.ds(pl.multiple_of(t * own + r * 16, 16), 16), :] = (
            f * scale * fg_ref[...]
        ).astype(BF16)

    vd_serve(3)
    nm_start()
    vd_serve(4)
    vd_serve(5)
    nm_middle()
    vd_serve(6)
    nm_end()
    vd_serve(7)
    nm_arrived()

    def w_bytes(a, rows, blocks, send, recv):
        ref = wbuf.at[a, pl.ds(0, rows), pl.ds(0, blocks * LANES)]
        return remote(ref, ref, send, recv, {"grp": partner})

    def y_arrived(a, step):
        if a == 0:
            w_bytes(0, units // 2, n_sp - 1, y_s.at[0], y_r.at[0]).wait_recv()
            return
        i = 1 + (a - 1) * half + step
        for last, count in ((False, 2), (True, 1)):

            @when((step == half - 1) == last)
            def _():
                w_bytes(a, private, count, y_s.at[a], y_r.at[i]).wait_recv()

    def halo_copy(direction):
        src = normed.at[pl.ds(tok - 8 if direction == 0 else 0, 8), :]
        dst = normed.at[pl.ds(tok + 8 * direction, 8), :]
        return remote(src, dst, halo_s, halo_r, z_device(direction))

    for direction in range(2):
        halo_copy(direction).start()
    if half >= 8:
        vd_serve(half)
    y_arrived(0, None)
    def halo_bytes():
        ref = normed.at[pl.ds(tok, 16), :]
        return remote(ref, ref, halo_s, halo_r, z_device(0))

    halo_bytes().wait_recv()

    m_rows = min(256, tok)
    m_count = tok // m_rows

    def put_up(a, made, i):
        made = made.astype(BF16).astype(F32)
        ups[a, pl.ds(8 + i * m_rows, m_rows), :] = made[:m_rows]
        if i == m_count - 1:
            ups[a, pl.ds(0, 8), :] = jnp.where(s == 0, 0.0, made[m_rows : m_rows + 8])
            ups[a, pl.ds(tok + 8, 8), :] = jnp.where(s == n_sp - 1, 0.0, made[m_rows + 8 :])

    def up_rows(i):
        return pl.ds(i * m_rows, m_rows + (16 if i == m_count - 1 else 0))

    for i in range(m_count):
        made = lax.dot_general(
            normed[up_rows(i), :],
            wbuf[0],
            (((1,), (1,)), ((), ())),
            preferred_element_type=F32,
        )
        put_up(0, made, i)

    done = half - d_lag if half >= 8 else half
    w_serve((2,), done + 1)

    c_rows = own // 2

    def convolved(a, taps, row):
        near = ups[a, pl.ds(pl.multiple_of(row, 8), c_rows + 16), :]
        return (
            taps[0:1, :] * near[7 : 7 + c_rows]
            + taps[1:2, :] * near[8 : 8 + c_rows]
            + taps[2:3, :] * near[9 : 9 + c_rows]
        )

    def blocks(j):
        return (s + n_sp - j) % n_sp, (s + j % half) % n_sp

    def cols(block):
        return pl.ds(pl.multiple_of(block * LANES, LANES), LANES)

    def up_value(j, fresh=False, last=False):
        pair = blocks(j)
        weights = jnp.concatenate([wbuf[1, :, cols(b)] for b in pair], axis=1)
        for i in range(m_count):
            tokens = jnp.concatenate([normed[up_rows(i), cols(b)] for b in pair], axis=1)
            made = lax.dot_general(
                tokens, weights, (((1,), (1,)), ((), ())), preferred_element_type=F32
            )
            if not fresh:
                made += partial_up[up_rows(i), :]
            if last:
                put_up(1, made, i)
            else:
                partial_up[up_rows(i), :] = made

    if half > 1:
        y_arrived(1, 0)
        up_value(1, fresh=True)

        @pl.loop(2, half)
        def _(j):
            y_arrived(1, j - 1)
            up_value(j)

            @pl.when(j == half // 2)
            def _():
                w_serve((2,), done + 2)

    w_serve((2,), done + 3)
    y_arrived(1, half - 1)
    up_value(half, last=True)
    done = min(done + 3, half) if half > 2 else half

    @pl.loop(0, 2 * n_tp)
    def _(i):
        to, lower = i // 2, i % 2
        v = convolved(0, cg_ref, i * c_rows)
        inner = (2.0 / np.pi) ** 0.5 * (v + 0.044715 * (v * v * v))
        gated = 0.5 * v * (1.0 + jnp.tanh(inner)) * convolved(1, cv_ref, i * c_rows)
        start = ((to % 2) * n_x + to // 2) * own + lower * c_rows
        hidden[pl.ds(pl.multiple_of(start, 8), c_rows), :] = gated.astype(BF16)

    per_core = n_x * own
    chips = ((x + 1) % n_x, (x + n_x - 1) % n_x)
    chip_far = (x + 2) % n_x
    toward = ({"tp": x_right}, {"tp": x_left})

    def rows_at(start, size):
        return pl.ds(pl.multiple_of(start, 16), size)

    def pair_copy(j, block, core):
        return remote(
            part.at[block, rows_at(core * per_core, per_core), :],
            pair_in.at[block],
            pair_s,
            pair_r.at[j - 1],
            {"tp": sibling},
        )

    def far_copy(j, direction, block):
        return remote(
            pair_sum.at[block, rows_at(chip_far * own, own), :],
            far_in.at[block],
            far_s,
            far_r.at[j - 1],
            toward[direction],
        )

    def near_copy(direction, block):
        return remote(
            pair_sum.at[block, rows_at(chips[direction] * own, own), :],
            near_in.at[direction, block],
            near_s,
            near_r,
            toward[direction],
        )

    def bytes_of(ref, send, recv):
        return remote(ref, ref, send, recv, {"tp": sibling})

    def pair_added(block, chip):
        mine = part[block, rows_at(c * per_core + chip * own, own), :]
        other = pair_in[block, rows_at(chip * own, own), :]
        return mine.astype(F32) + other.astype(F32)

    sum_lag, send_lag = 1, 3

    @pl.loop(1, half + send_lag + 1)
    def _(j):
        @pl.when(j <= half)
        def _():
            @pl.when(j > done)
            def _():
                w_serve((2,), j)

            y_arrived(2, j - 1)
            first, second = blocks(j)
            both = jnp.concatenate([wbuf[2, :, cols(first)], wbuf[2, :, cols(second)]], axis=1)

            @pl.loop(0, m_count, unroll=True)
            def _(i):
                rows = pl.ds(pl.multiple_of(i * m_rows, m_rows), m_rows)
                made = jnp.dot(hidden[rows, :], both, preferred_element_type=F32).astype(BF16)
                part[first, rows, :] = made[:, :LANES]
                part[second, rows, :] = made[:, LANES:]

            for block in (first, second):
                pair_copy(j, block, 1 - c).start()

        @pl.when((j > sum_lag) & (j <= half + sum_lag))
        def _():
            two = pair_in.at[pl.ds(0, 2)]
            bytes_of(two, pair_s, pair_r.at[j - sum_lag - 1]).wait_recv()
            for direction, block in enumerate(blocks(j - sum_lag)):
                for chip in (chip_far, chips[1 - direction]):
                    pair_sum[block, rows_at(chip * own, own), :] = pair_added(block, chip).astype(
                        BF16
                    )
                far_copy(j - sum_lag, direction, block).start()
                near_copy(1 - direction, block).start()

        @pl.when(j > send_lag)
        def _():
            two = far_in.at[pl.ds(0, 2)]
            bytes_of(two, far_s, far_r.at[j - send_lag - 1]).wait_recv()
            for direction, block in enumerate(blocks(j - send_lag)):
                chip = chips[direction]
                pair_sum[block, rows_at(chip * own, own), :] = (
                    pair_added(block, chip) + far_in[block].astype(F32)
                ).astype(BF16)
                near_copy(direction, block).start()

    bytes_of(near_in, near_s, near_r).wait_recv()

    for b in range(n_sp):
        span = slice(b * LANES, (b + 1) * LANES)
        total = pair_added(b, x)
        for direction in range(2):
            total += near_in[direction, b].astype(F32)
        out_ref[:, span] = (stream[:, span].astype(F32) + total).astype(BF16)

    ow_bytes(2 * n_x - 1).wait_send()
    nm_sent()
    att_bytes().wait_send()
    halo_bytes().wait_send()
    bytes_of(pair_in, pair_s, pair_r.at[0]).wait_send()
    bytes_of(far_in, far_s, far_r.at[0]).wait_send()
    bytes_of(near_in, near_s, near_r).wait_send()
    turns = n_sp - 1

    def kv_bytes(rows, send):
        ref = kv.at[0, pl.ds(0, rows), :]
        return remote(ref, ref, send, sib_r.at[0], {"tp": sibling})

    kv_bytes(turns * (kv_private + kv_common), kv_s).wait_send()
    kv_bytes(turns * kv_private, xp_s).wait_send()
    kv_bytes(turns * tok, sib_s).wait_send()
    for a in range(3):
        along = units // 2 if a == 0 else private + common
        over = units // 2 if a == 0 else private
        w_bytes(a, along, turns, w_s.at[a], w_r.at[0]).wait_send()
        w_bytes(a, over, turns, y_s.at[a], y_r.at[0]).wait_send()


def body(
    queries,
    keys,
    values,
    query_gain,
    key_gain,
    residual,
    out_weight,
    mix_gain,
    ffn_gain,
    gate_in,
    value_in,
    conv_gate,
    conv_value,
    down_t,
):
    n_sp, n_tp = lax.axis_size("sp"), lax.axis_size("tp")
    half = n_sp // 2
    tok = queries.shape[0]
    own, model = residual.shape
    units = gate_in.shape[1]
    row_tab, col_tab = rotary_tables(tok * n_sp, query_gain.shape[0])
    vmem = pl.BlockSpec(memory_space=pltpu.VMEM)
    dma = pltpu.SemaphoreType.DMA
    operands = (
        jnp.asarray(row_tab),
        jnp.asarray(col_tab),
        queries,
        keys,
        values,
        query_gain[None, :],
        key_gain[None, :],
        residual,
        out_weight,
        mix_gain[None, :],
        ffn_gain[None, :],
        gate_in.T,
        value_in.T,
        down_t.T,
        conv_gate,
        conv_value,
    )
    return pl.pallas_call(
        functools.partial(ring_kernel, n_sp, n_tp),
        out_shape=jax.ShapeDtypeStruct((own, model), BF16),
        in_specs=[vmem] * len(operands),
        out_specs=vmem,
        scratch_shapes=[
            pltpu.VMEM((2, tok * n_sp, LANES), BF16),
            pltpu.VMEM((tok, LANES), BF16),
            pltpu.VMEM((tok, LANES), F32),
            pltpu.VMEM((tok, LANES), F32),
            pltpu.VMEM((tok, LANES), F32),
            pltpu.VMEM((tok, LANES), BF16),
            pltpu.VMEM((own, n_tp * LANES), BF16),
            pltpu.VMEM((n_tp * out_weight.shape[0], model), BF16),
            pltpu.VMEM((own, model), F32),
            pltpu.VMEM((own, model), BF16),
            pltpu.VMEM((tok + 16, model), BF16),
            pltpu.VMEM((3, units, model), BF16),
            pltpu.VMEM((2, tok + 16, units), F32),
            pltpu.VMEM((tok + 16, units), F32),
            pltpu.VMEM((tok, units), BF16),
            pltpu.VMEM((n_sp, tok, LANES), BF16),
            pltpu.VMEM((n_sp, tok // 2, LANES), BF16),
            pltpu.VMEM((n_sp, tok // 2, LANES), BF16),
            pltpu.VMEM((n_sp, own, LANES), BF16),
            pltpu.VMEM((2, n_sp, own, LANES), BF16),
            dma,
            dma((4 * half,)),
            dma,
            dma((2 * half,)),
            dma,
            dma((2 * half,)),
            dma((3,)),
            dma((12 * half,)),
            dma((3,)),
            dma((2 * half + 1,)),
            dma,
            dma((2 * (out_weight.shape[0] // 16) + 2,)),
            dma,
            dma((5,)),
            dma,
            dma,
            dma,
            dma,
            dma,
            dma((half,)),
            dma,
            dma((half,)),
            dma,
            dma,
        ],
        compiler_params=pltpu.CompilerParams(
            collective_id=0,
            has_side_effects=True,
            vmem_limit_bytes=62 * 1024 * 1024,
        ),
        name="layer",
    )(*operands)


def solution(mesh):
    return jax.shard_map(
        body,
        mesh=mesh,
        in_specs=(
            P(("grp", "sp"), "tp"),
            P(("grp", "sp"), None),
            P(("grp", "sp"), None),
            P(),
            P(),
            P(("grp", "sp", "tp"), None),
            P("tp", None),
            P(),
            P(),
            P("sp", "tp"),
            P("sp", "tp"),
            P(None, "tp"),
            P(None, "tp"),
            P("sp", "tp"),
        ),
        out_specs=P(("grp", "sp", "tp"), None),
        check_vma=False,
    )
```

```python
import functools

import jax
import jax.numpy as jnp
import numpy as np
from jax import lax
from jax.experimental import pallas as pl
from jax.experimental.pallas import tpu as pltpu
from jax.sharding import PartitionSpec as P

HEADS = 8
KVH = 2
GRID_W = 64
EPSILON = 1e-06
THETA = 10000.0
LANES = 128
MESH = pl.DeviceIdType.MESH
F32 = jnp.float32
BF16 = jnp.bfloat16


def rotary_tables(seq_total, head_dim):
    quarter = head_dim // 4
    inverse = np.float32(THETA) ** (
        -(np.float32(2.0) * np.arange(quarter, dtype=np.float32)) / np.float32(head_dim // 2)
    )
    inverse = inverse.astype(np.float32)
    rows = (np.arange(seq_total // GRID_W) - seq_total // GRID_W // 2).astype(np.float32)
    cols = (np.arange(GRID_W) - GRID_W // 2).astype(np.float32)
    sign = np.where((np.arange(head_dim) // quarter) % 2 == 0, -1.0, 1.0).astype(np.float32)

    def tables(positions):
        angle = np.tile((positions[:, None] * inverse[None, :]).astype(np.float32), (1, 4))
        angle = angle.astype(np.float64)
        return np.stack([np.cos(angle), np.sin(angle) * sign]).astype(np.float32)

    return tables(rows), tables(cols)


def ring_kernel(
    n_sp,
    n_tp,
    row_tab,
    col_tab,
    q_ref,
    k_ref,
    v_ref,
    qg_ref,
    kg_ref,
    res_ref,
    ow_ref,
    mg_ref,
    fg_ref,
    g_ref,
    u_ref,
    d_ref,
    cg_ref,
    cv_ref,
    out_ref,
    kv,
    q_rot,
    top,
    den,
    acc,
    att_own,
    att_all,
    ow_all,
    mix,
    stream,
    normed,
    wbuf,
    ups,
    partial_up,
    hidden,
    part,
    pair_in,
    pair_sum,
    far_in,
    near_in,
    kv_s,
    kv_r,
    sib_s,
    sib_r,
    xp_s,
    xp_r,
    w_s,
    w_r,
    y_s,
    y_r,
    ow_s,
    ow_r,
    nm_s,
    nm_r,
    a2a_s,
    a2a_r,
    halo_s,
    halo_r,
    pair_s,
    pair_r,
    far_s,
    far_r,
    near_s,
    near_r,
):
    half = n_sp // 2
    n_x = n_tp // 2
    tok = q_ref.shape[0]
    own = res_ref.shape[0]
    model = res_ref.shape[1]
    units = g_ref.shape[0]
    common = units * 4 // 11 // 16 * 16
    private = (units - common) // 2
    kv_common = tok // 4 // 32 * 32
    kv_private = (tok - kv_common) // 2
    sources = (g_ref, u_ref, d_ref)

    g = lax.axis_index("grp")
    s = lax.axis_index("sp")
    t = lax.axis_index("tp")
    x, c = t // 2, t % 2
    z_right, z_left = (s + 1) % n_sp, (s + n_sp - 1) % n_sp
    partner = g + 1 - 2 * (g % 2)
    sibling = t + 1 - 2 * c
    x_right = 2 * ((x + 1) % n_x) + c
    x_left = 2 * ((x + n_x - 1) % n_x) + c
    kv_head = t // (HEADS // KVH)
    x_pair = x + 1 - 2 * (x % 2)
    x_cross = (x + n_x - 1 + 2 * (x % 2)) % n_x

    barrier = pltpu.get_barrier_semaphore()
    peers = [{"sp": z_right}, {"sp": z_left}, {"grp": partner}]
    peers += [{"tp": (t + i) % n_tp} for i in range(1, n_tp)]
    for peer in peers:
        pl.semaphore_signal(barrier, inc=1, device_id=peer, device_id_type=MESH)

    def remote(src, dst, send, recv, device):
        return pltpu.make_async_remote_copy(
            src_ref=src,
            dst_ref=dst,
            send_sem=send,
            recv_sem=recv,
            device_id=device,
            device_id_type=MESH,
        )

    def block_of(direction, step):
        return (s + n_sp - step) % n_sp if direction == 0 else (s + step) % n_sp

    def z_device(direction):
        return {"sp": z_right if direction == 0 else z_left}

    def kv_at(which, block, piece, side):
        if piece == 0:
            start, size = side * (kv_private + kv_common), kv_private
        else:
            start, size = kv_private, kv_common
        return kv.at[which, pl.ds(pl.multiple_of(block * tok + start, 16), size), :]

    def kv_copy(direction, step, piece, block):
        ref = kv_at(c, block, piece, x % 2)
        i = (direction * half + step) * 2 + piece
        return remote(ref, ref, kv_s, kv_r.at[i], z_device(direction))

    def sib_copy(which, direction, step, piece, block):
        ref = kv_at(which, block, piece, x % 2)
        i = jnp.where(step == half - 1, 0, direction) * half + step
        return remote(ref, ref, sib_s, sib_r.at[i], {"tp": sibling})

    def xp_copy(direction, step, block, mine):
        ref = kv_at(c, block, 0, x % 2 if mine else 1 - x % 2)
        i = direction * half + step
        return remote(ref, ref, xp_s, xp_r.at[i], {"tp": 2 * x_pair + c})

    def rel_copy(which, direction, step, block):
        ref = kv_at(which, block, 0, 1 - x % 2)
        i = direction * half + step
        return remote(ref, ref, sib_s, sib_r.at[i], {"tp": sibling})

    def sib_block(which, direction, step, block):
        ref = kv.at[which, pl.ds(pl.multiple_of(block * tok, tok), tok), :]
        i = direction * half + step
        return remote(ref, ref, sib_s, sib_r.at[i], {"tp": sibling})

    def w_rows(a, piece, side):
        if a == 0:
            start, size = side * (units // 2) + piece * (units // 4), units // 4
        elif piece == 0:
            start, size = side * (private + common), private
        else:
            start, size = private, common
        return pl.ds(pl.multiple_of(start, 16), size)

    def over_y(a, piece):
        return a == 0 or piece == 0

    def w_at(a, block, rows):
        return wbuf.at[a, rows, pl.ds(pl.multiple_of(block * LANES, LANES), LANES)]

    def w_copy(a, direction, step, piece, block, first=False):
        rows = w_rows(a, piece, g % 2)
        dst = w_at(a, block, rows)
        src = sources[a].at[rows, :] if first else dst
        i = ((a * 2 + direction) * half + step) * 2 + piece
        return remote(src, dst, w_s.at[a], w_r.at[i], z_device(direction))

    def y_copy(a, direction, step, piece, block, mine):
        ref = w_at(a, block, w_rows(a, piece, g % 2 if mine else 1 - g % 2))
        i = 0 if a == 0 else 1 + (a - 1) * half + step
        return remote(ref, ref, y_s.at[a], y_r.at[i], {"grp": partner})

    def w_start(arrays):
        for piece in range(2):
            for a in arrays:
                for direction in range(2):
                    w_copy(a, direction, 0, piece, s, first=True).start()

    def when(condition):
        if isinstance(condition, bool):
            return (lambda f: f()) if condition else (lambda f: None)
        return pl.when(condition)

    def w_serve(arrays, k, pieces=(0, 1)):
        for piece in pieces:
            for a in arrays:
                for direction in range(2):
                    last = direction == piece
                    block = block_of(direction, k)

                    @when((k >= 1) & (k <= half if last else k < half))
                    def _():
                        w_copy(a, direction, k - 1, piece, block).wait_recv()

                        @when(k <= half - 1 if last else k <= half - 2)
                        def _():
                            w_copy(a, direction, k, piece, block).start()

                        if over_y(a, piece):
                            y_copy(a, direction, k - 1, piece, block, True).start()

    def x_gather(buf, rows, first, send, recv):
        hold = rows // 2

        def at(block, lo, size):
            return buf.at[pl.ds(pl.multiple_of(block * rows + lo, 16), size), :]

        def ring(direction, step, chip, lo, size, src=None):
            dst = at(2 * chip + c, lo, size)
            i = direction * 2 + step
            device = {"tp": x_right if direction == 0 else x_left}
            return remote(dst if src is None else src, dst, send, recv.at[i], device)

        def share(chip, core, lo, size, src=None):
            dst = at(2 * chip + core, lo, size)
            return remote(
                dst if src is None else src, dst, send, recv.at[4], {"tp": sibling}
            )

        chips = ((x + n_x - 1) % n_x, (x + 1) % n_x)
        far = (x + 2) % n_x

        def start():
            for direction in range(2):
                ring(direction, 0, x, 0, rows, first).start()
            share(x, c, 0, rows, first).start()

        def middle():
            for direction in range(2):
                chip = chips[direction]
                ring(direction, 0, chip, 0, rows).wait_recv()
                ring(direction, 1, chip, direction * hold, hold).start()
                share(chip, c, 0, rows).start()

        def end():
            for direction in range(2):
                ring(direction, 1, far, direction * hold, hold).wait_recv()
                share(far, c, direction * hold, hold).start()

        def all_rows(blocks):
            ref = buf.at[pl.ds(0, blocks * rows), :]
            return remote(ref, ref, send, recv.at[4], {"tp": sibling})

        def arrived():
            all_rows(n_x).wait_recv()

        def sent():
            all_rows(2 * n_x - 1).wait_send()

        return start, middle, end, arrived, sent

    ow_rows = ow_ref.shape[0]
    ow_parts = ow_rows // 16
    ow_far = x_cross + 1 - 2 * (x_cross % 2)

    def ow_copy(i, chip, core, lo, size, device, first=False):
        dst = ow_all.at[pl.ds(pl.multiple_of((2 * chip + core) * ow_rows + lo, 16), size), :]
        src = ow_ref.at[pl.ds(lo, size), :] if first else dst
        return remote(src, dst, ow_s, ow_r.at[i], {"tp": device})

    size = ow_rows // ow_parts

    def ow_pair(q, chip, first=False):
        return ow_copy(q, chip, c, q * size, size, 2 * x_pair + c, first)

    def ow_over(chip, first=False):
        return ow_copy(ow_parts, chip, c, 0, ow_rows, 2 * x_cross + c, first)

    def ow_on(q, chip):
        return ow_copy(ow_parts + 1 + q, chip, c, q * size, size, 2 * x_cross + c)

    def ow_own(core, first=False):
        return ow_copy(2 * ow_parts + 1, x, core, 0, ow_rows, sibling, first)

    def ow_share(i, chip, core, lo, size):
        return ow_copy(2 * ow_parts + 1, chip, core, lo, size, sibling)

    def ow_shares(core, i):
        if i == ow_parts:
            return ow_share(i, x_cross, core, 0, ow_rows)
        if i < ow_parts:
            return ow_share(i, x_pair, core, i * size, size)
        return ow_share(i, ow_far, core, (i - ow_parts - 1) * size, size)

    def ow_bytes(blocks):
        ref = ow_all.at[pl.ds(0, blocks * ow_rows), :]
        return remote(ref, ref, ow_s, ow_r.at[2 * ow_parts + 1], {"tp": sibling})

    def ow_take(q):
        ow_pair(q, x_pair).wait_recv()
        ow_on(q, x_pair).start()
        ow_shares(c, q).start()

    def ow_across():
        ow_over(x_cross).wait_recv()
        ow_shares(c, ow_parts).start()

    def ow_take_far(q):
        ow_on(q, ow_far).wait_recv()
        ow_shares(c, ow_parts + 1 + q).start()

    nm_start, nm_middle, nm_end, nm_arrived, nm_sent = x_gather(normed, own, None, nm_s, nm_r)

    grid_rows = tok // GRID_W
    lane = lax.broadcasted_iota(jnp.int32, (GRID_W, LANES), 1)
    quarter = LANES // 4

    def prepare(raw, gain, grid_row, factor):
        floats = raw.astype(F32)
        mean = jnp.sum(floats * floats, axis=-1, keepdims=True) * (1.0 / LANES)
        n = floats * lax.rsqrt(mean + EPSILON) * gain
        at = s * grid_rows + grid_row
        cos = jnp.where(lane < LANES // 2, row_tab[0, pl.ds(at, 1), :], col_tab[0])
        sin = jnp.where(lane < LANES // 2, row_tab[1, pl.ds(at, 1), :], col_tab[1])
        turned = jnp.where(
            (lane // quarter) % 2 == 0,
            pltpu.roll(n, LANES - quarter, 1),
            pltpu.roll(n, quarter, 1),
        )
        return ((n * cos + turned * sin) * factor).astype(BF16)

    head_cols = pl.ds(pl.multiple_of(kv_head * LANES, LANES), LANES)

    @pl.loop(0, grid_rows)
    def _(r):
        rows = pl.ds(pl.multiple_of(r * GRID_W, GRID_W), GRID_W)
        into = pl.ds(pl.multiple_of(s * tok + r * GRID_W, GRID_W), GRID_W)
        kv[0, into, :] = prepare(k_ref[rows, head_cols], kg_ref[...], r, 1.0)
        kv[1, into, :] = v_ref[rows, head_cols]

    pl.semaphore_wait(barrier, len(peers))
    for piece in range(2):
        for direction in range(2):
            kv_copy(direction, 0, piece, s).start()
    ow_over(x, first=True).start()
    ow_own(c, first=True).start()
    w_start((0,))

    @pl.loop(0, grid_rows)
    def _(r):
        rows = pl.ds(pl.multiple_of(r * GRID_W, GRID_W), GRID_W)
        q_rot[rows, :] = prepare(q_ref[rows, :], qg_ref[...], r, LANES ** (-0.5))

    top[...] = jnp.full_like(top, -1e30)
    den[...] = jnp.zeros_like(den)
    acc[...] = jnp.zeros_like(acc)
    for a in range(3):
        wbuf[a, :, pl.ds(pl.multiple_of(s * LANES, LANES), LANES)] = sources[a][...]
    ow_all[pl.ds(pl.multiple_of(t * ow_rows, 16), ow_rows), :] = ow_ref[...]

    chunk = min(256, tok)

    def attend(block):
        keys = pl.ds(pl.multiple_of(block * tok, tok), tok)

        @pl.loop(0, tok // chunk, unroll=True)
        def _(i):
            rows = pl.ds(pl.multiple_of(i * chunk, chunk), chunk)
            scores = lax.dot_general(
                q_rot[rows, :],
                kv[0, keys, :],
                (((1,), (1,)), ((), ())),
                preferred_element_type=F32,
            )
            before = top[rows, :]
            newest = jnp.maximum(before, jnp.max(scores, axis=1, keepdims=True))
            wide = jnp.concatenate([newest] * (tok // LANES), axis=1)
            weights = jnp.exp(scores - wide)
            fade = jnp.exp(before - newest)
            den[rows, :] = den[rows, :] * fade + jnp.sum(weights, axis=1, keepdims=True)
            acc[rows, :] = acc[rows, :] * fade + jnp.dot(
                weights.astype(BF16), kv[1, keys, :], preferred_element_type=F32
            )
            top[rows, :] = newest

    ow_in_loop = min(ow_parts, max(half - 4, 0))
    @pl.loop(1, half + 3)
    def _(k):
        def at_step(step, act):
            @pl.when(k == min(step, half + 2))
            def _():
                act()

        def kv_serve(piece):
            for direction in range(2):
                last = direction == piece
                block = block_of(direction, k)

                @pl.when(k <= half if last else k < half)
                def _():
                    kv_copy(direction, k - 1, piece, block).wait_recv()

                    @pl.when(k <= half - 1 if last else k <= half - 2)
                    def _():
                        kv_copy(direction, k, piece, block).start()

                    if piece == 0:
                        xp_copy(direction, k - 1, block, True).start()
                    sib_copy(c, direction, k - 1, piece, block).start()

        kv_serve(0)
        for q in range(ow_parts):
            at_step(1 + q, lambda: ow_pair(q, x, first=True).start())
        w_serve((0,), k - 1, (0,))
        for direction in range(2):
            block = block_of(direction, k - 1)

            @pl.when((k >= 2) & (k <= half + 1 if direction == 0 else k <= half))
            def _():
                xp_copy(direction, k - 2, block, False).wait_recv()
                rel_copy(c, direction, k - 2, block).start()

        for direction in range(2):
            block = block_of(direction, k - 2)

            @pl.when((k >= 3) & (k <= half + 2 if direction == 0 else k <= half + 1))
            def _():
                sib_block(1 - c, direction, k - 3, block).wait_recv()

        @pl.when(k != 2)
        def _():
            attend((s + n_sp - jnp.where(k == 1, 0, k - 2)) % n_sp)

        kv_serve(1)
        w_serve((0,), k - 1, (1,))
        for q in range(ow_parts):
            at_step(3 + q, lambda: ow_take(q))
        at_step(5, ow_across)
        for q in range(ow_in_loop):
            at_step(6 + q, lambda: ow_take_far(q))
        at_step(half, lambda: w_start((1,)))

        @pl.when((k >= 3) & (k <= half + 1))
        def _():
            attend((s + k - 2) % n_sp)

        at_step(half + 2, lambda: w_serve((1,), 1))

    d_lag = 2

    def vd_serve(k):
        for piece in range(2):
            w_serve((1,), k, (piece,))
            w_serve((2,), k - d_lag, (piece,))
        if k == d_lag:
            w_start((2,))

    att_own[...] = (acc[...] / den[...]).astype(BF16)

    def att_copy(to, source):
        cols = pl.ds(pl.multiple_of(source * LANES, LANES), LANES)
        rows = pl.ds(pl.multiple_of(to * own, 16), own)
        return remote(
            att_own.at[rows, :],
            att_all.at[:, cols],
            a2a_s,
            a2a_r,
            {"tp": to},
        )

    for i in range(1, n_tp):
        att_copy((t + i) % n_tp, t).start()
    att_all[:, pl.ds(pl.multiple_of(t * LANES, LANES), LANES)] = att_own[
        pl.ds(pl.multiple_of(t * own, 16), own), :
    ]
    vd_serve(2)
    for q in range(ow_in_loop, ow_parts):
        ow_take_far(q)
    ow_bytes(n_x).wait_recv()
    def att_bytes():
        ref = att_all.at[:, pl.ds(0, (n_tp - 1) * LANES)]
        return remote(ref, ref, a2a_s, a2a_r, {"tp": sibling})

    att_bytes().wait_recv()

    width = min(512, model)

    @pl.loop(0, model // width)
    def _(j):
        cols = pl.ds(pl.multiple_of(j * width, width), width)
        total = jnp.zeros((own, width), F32)
        for head in range(n_tp):
            span = slice(head * LANES, (head + 1) * LANES)
            total += (
                jnp.dot(att_all[:, span], ow_all[span, cols], preferred_element_type=F32)
                .astype(BF16)
                .astype(F32)
            )
        mix[:, cols] = total

    @pl.loop(0, own // 16)
    def _(r):
        rows = pl.ds(pl.multiple_of(r * 16, 16), 16)
        m = mix[rows, :]
        scale = lax.rsqrt(jnp.mean(m * m, axis=-1, keepdims=True) + EPSILON)
        added = (res_ref[rows, :].astype(F32) + m * scale * mg_ref[...]).astype(BF16)
        stream[rows, :] = added
        f = added.astype(F32)
        scale = lax.rsqrt(jnp.mean(f * f, axis=-1, keepdims=True) + EPSILON)
        normed[pl.ds(pl.multiple_of(t * own + r * 16, 16), 16), :] = (
            f * scale * fg_ref[...]
        ).astype(BF16)

    vd_serve(3)
    nm_start()
    vd_serve(4)
    vd_serve(5)
    nm_middle()
    vd_serve(6)
    nm_end()
    vd_serve(7)
    nm_arrived()

    def w_bytes(a, rows, blocks, send, recv):
        ref = wbuf.at[a, pl.ds(0, rows), pl.ds(0, blocks * LANES)]
        return remote(ref, ref, send, recv, {"grp": partner})

    def y_arrived(a, step):
        if a == 0:
            w_bytes(0, units // 2, n_sp - 1, y_s.at[0], y_r.at[0]).wait_recv()
            return
        i = 1 + (a - 1) * half + step
        for last, count in ((False, 2), (True, 1)):

            @when((step == half - 1) == last)
            def _():
                w_bytes(a, private, count, y_s.at[a], y_r.at[i]).wait_recv()

    def halo_copy(direction):
        src = normed.at[pl.ds(tok - 8 if direction == 0 else 0, 8), :]
        dst = normed.at[pl.ds(tok + 8 * direction, 8), :]
        return remote(src, dst, halo_s, halo_r, z_device(direction))

    for direction in range(2):
        halo_copy(direction).start()
    y_arrived(0, None)
    def halo_bytes():
        ref = normed.at[pl.ds(tok, 16), :]
        return remote(ref, ref, halo_s, halo_r, z_device(0))

    m_rows = min(256, tok)
    m_count = tok // m_rows

    def put_up(a, made, i):
        made = made.astype(BF16).astype(F32)
        ups[a, pl.ds(8 + i * m_rows, m_rows), :] = made[:m_rows]
        if i == m_count - 1:
            ups[a, pl.ds(0, 8), :] = jnp.where(s == 0, 0.0, made[m_rows : m_rows + 8])
            ups[a, pl.ds(tok + 8, 8), :] = jnp.where(s == n_sp - 1, 0.0, made[m_rows + 8 :])

    def up_rows(i):
        return pl.ds(i * m_rows, m_rows + (16 if i == m_count - 1 else 0))

    for i in range(m_count):
        if i == m_count - 1:
            halo_bytes().wait_recv()
        made = lax.dot_general(
            normed[up_rows(i), :],
            wbuf[0],
            (((1,), (1,)), ((), ())),
            preferred_element_type=F32,
        )
        put_up(0, made, i)

    if half >= 8:
        vd_serve(half)
    done = half - d_lag if half >= 8 else half

    c_rows = own // 2

    def convolved(a, taps, row):
        near = ups[a, pl.ds(pl.multiple_of(row, 8), c_rows + 16), :]
        return (
            taps[0:1, :] * near[7 : 7 + c_rows]
            + taps[1:2, :] * near[8 : 8 + c_rows]
            + taps[2:3, :] * near[9 : 9 + c_rows]
        )

    def blocks(j):
        return (s + n_sp - j) % n_sp, (s + j % half) % n_sp

    def cols(block):
        return pl.ds(pl.multiple_of(block * LANES, LANES), LANES)

    def up_value(j, fresh=False, last=False):
        pair = blocks(j)
        weights = jnp.concatenate([wbuf[1, :, cols(b)] for b in pair], axis=1)
        for i in range(m_count):
            tokens = jnp.concatenate([normed[up_rows(i), cols(b)] for b in pair], axis=1)
            made = lax.dot_general(
                tokens, weights, (((1,), (1,)), ((), ())), preferred_element_type=F32
            )
            if not fresh:
                made += partial_up[up_rows(i), :]
            if last:
                put_up(1, made, i)
            else:
                partial_up[up_rows(i), :] = made

    if half > 1:
        y_arrived(1, 0)
        up_value(1, fresh=True)

        @pl.loop(2, half)
        def _(j):
            y_arrived(1, j - 1)
            up_value(j)

    y_arrived(1, half - 1)
    up_value(half, last=True)
    w_serve((2,), done + 1)
    done = min(done + 1, half)

    @pl.loop(0, 2 * n_tp)
    def _(i):
        to, lower = i // 2, i % 2
        v = convolved(0, cg_ref, i * c_rows)
        inner = (2.0 / np.pi) ** 0.5 * (v + 0.044715 * (v * v * v))
        gated = 0.5 * v * (1.0 + jnp.tanh(inner)) * convolved(1, cv_ref, i * c_rows)
        start = ((to % 2) * n_x + to // 2) * own + lower * c_rows
        hidden[pl.ds(pl.multiple_of(start, 8), c_rows), :] = gated.astype(BF16)

    w_serve((2,), done + 1)
    done = min(done + 1, half)

    per_core = n_x * own
    chips = ((x + 1) % n_x, (x + n_x - 1) % n_x)
    chip_far = (x + 2) % n_x
    toward = ({"tp": x_right}, {"tp": x_left})

    def rows_at(start, size):
        return pl.ds(pl.multiple_of(start, 16), size)

    def pair_copy(j, block, core):
        return remote(
            part.at[block, rows_at(core * per_core, per_core), :],
            pair_in.at[block],
            pair_s,
            pair_r.at[j - 1],
            {"tp": sibling},
        )

    def far_copy(j, direction, block):
        return remote(
            pair_sum.at[block, rows_at(chip_far * own, own), :],
            far_in.at[block],
            far_s,
            far_r.at[j - 1],
            toward[direction],
        )

    def near_copy(direction, block):
        return remote(
            pair_sum.at[block, rows_at(chips[direction] * own, own), :],
            near_in.at[direction, block],
            near_s,
            near_r,
            toward[direction],
        )

    def bytes_of(ref, send, recv):
        return remote(ref, ref, send, recv, {"tp": sibling})

    def pair_added(block, chip):
        mine = part[block, rows_at(c * per_core + chip * own, own), :]
        other = pair_in[block, rows_at(chip * own, own), :]
        return mine.astype(F32) + other.astype(F32)

    sum_lag, send_lag = 1, 3

    @pl.loop(1, half + send_lag + 1)
    def _(j):
        @pl.when(j <= half)
        def _():
            @pl.when(j > done)
            def _():
                w_serve((2,), j)

            y_arrived(2, j - 1)
            first, second = blocks(j)
            both = jnp.concatenate([wbuf[2, :, cols(first)], wbuf[2, :, cols(second)]], axis=1)

            @pl.loop(0, m_count, unroll=True)
            def _(i):
                rows = pl.ds(pl.multiple_of(i * m_rows, m_rows), m_rows)
                made = jnp.dot(hidden[rows, :], both, preferred_element_type=F32).astype(BF16)
                part[first, rows, :] = made[:, :LANES]
                part[second, rows, :] = made[:, LANES:]

            for block in (first, second):
                pair_copy(j, block, 1 - c).start()

        @pl.when((j > sum_lag) & (j <= half + sum_lag))
        def _():
            two = pair_in.at[pl.ds(0, 2)]
            bytes_of(two, pair_s, pair_r.at[j - sum_lag - 1]).wait_recv()
            for direction, block in enumerate(blocks(j - sum_lag)):
                for chip in (chip_far, chips[1 - direction]):
                    pair_sum[block, rows_at(chip * own, own), :] = pair_added(block, chip).astype(
                        BF16
                    )
                far_copy(j - sum_lag, direction, block).start()
                near_copy(1 - direction, block).start()

        @pl.when(j > send_lag)
        def _():
            two = far_in.at[pl.ds(0, 2)]
            bytes_of(two, far_s, far_r.at[j - send_lag - 1]).wait_recv()
            for direction, block in enumerate(blocks(j - send_lag)):
                chip = chips[direction]
                pair_sum[block, rows_at(chip * own, own), :] = (
                    pair_added(block, chip) + far_in[block].astype(F32)
                ).astype(BF16)
                near_copy(direction, block).start()

    bytes_of(near_in, near_s, near_r).wait_recv()

    for b in range(n_sp):
        span = slice(b * LANES, (b + 1) * LANES)
        total = pair_added(b, x)
        for direction in range(2):
            total += near_in[direction, b].astype(F32)
        out_ref[:, span] = (stream[:, span].astype(F32) + total).astype(BF16)

    ow_bytes(2 * n_x - 1).wait_send()
    nm_sent()
    att_bytes().wait_send()
    halo_bytes().wait_send()
    bytes_of(pair_in, pair_s, pair_r.at[0]).wait_send()
    bytes_of(far_in, far_s, far_r.at[0]).wait_send()
    bytes_of(near_in, near_s, near_r).wait_send()
    turns = n_sp - 1

    def kv_bytes(rows, send):
        ref = kv.at[0, pl.ds(0, rows), :]
        return remote(ref, ref, send, sib_r.at[0], {"tp": sibling})

    kv_bytes(turns * (kv_private + kv_common), kv_s).wait_send()
    kv_bytes(turns * kv_private, xp_s).wait_send()
    kv_bytes(turns * tok, sib_s).wait_send()
    for a in range(3):
        along = units // 2 if a == 0 else private + common
        over = units // 2 if a == 0 else private
        w_bytes(a, along, turns, w_s.at[a], w_r.at[0]).wait_send()
        w_bytes(a, over, turns, y_s.at[a], y_r.at[0]).wait_send()


def body(
    queries,
    keys,
    values,
    query_gain,
    key_gain,
    residual,
    out_weight,
    mix_gain,
    ffn_gain,
    gate_in,
    value_in,
    conv_gate,
    conv_value,
    down_t,
):
    n_sp, n_tp = lax.axis_size("sp"), lax.axis_size("tp")
    half = n_sp // 2
    tok = queries.shape[0]
    own, model = residual.shape
    units = gate_in.shape[1]
    row_tab, col_tab = rotary_tables(tok * n_sp, query_gain.shape[0])
    vmem = pl.BlockSpec(memory_space=pltpu.VMEM)
    dma = pltpu.SemaphoreType.DMA
    operands = (
        jnp.asarray(row_tab),
        jnp.asarray(col_tab),
        queries,
        keys,
        values,
        query_gain[None, :],
        key_gain[None, :],
        residual,
        out_weight,
        mix_gain[None, :],
        ffn_gain[None, :],
        gate_in.T,
        value_in.T,
        down_t.T,
        conv_gate,
        conv_value,
    )
    return pl.pallas_call(
        functools.partial(ring_kernel, n_sp, n_tp),
        out_shape=jax.ShapeDtypeStruct((own, model), BF16),
        in_specs=[vmem] * len(operands),
        out_specs=vmem,
        scratch_shapes=[
            pltpu.VMEM((2, tok * n_sp, LANES), BF16),
            pltpu.VMEM((tok, LANES), BF16),
            pltpu.VMEM((tok, LANES), F32),
            pltpu.VMEM((tok, LANES), F32),
            pltpu.VMEM((tok, LANES), F32),
            pltpu.VMEM((tok, LANES), BF16),
            pltpu.VMEM((own, n_tp * LANES), BF16),
            pltpu.VMEM((n_tp * out_weight.shape[0], model), BF16),
            pltpu.VMEM((own, model), F32),
            pltpu.VMEM((own, model), BF16),
            pltpu.VMEM((tok + 16, model), BF16),
            pltpu.VMEM((3, units, model), BF16),
            pltpu.VMEM((2, tok + 16, units), F32),
            pltpu.VMEM((tok + 16, units), F32),
            pltpu.VMEM((tok, units), BF16),
            pltpu.VMEM((n_sp, tok, LANES), BF16),
            pltpu.VMEM((n_sp, tok // 2, LANES), BF16),
            pltpu.VMEM((n_sp, tok // 2, LANES), BF16),
            pltpu.VMEM((n_sp, own, LANES), BF16),
            pltpu.VMEM((2, n_sp, own, LANES), BF16),
            dma,
            dma((4 * half,)),
            dma,
            dma((2 * half,)),
            dma,
            dma((2 * half,)),
            dma((3,)),
            dma((12 * half,)),
            dma((3,)),
            dma((2 * half + 1,)),
            dma,
            dma((2 * (out_weight.shape[0] // 16) + 2,)),
            dma,
            dma((5,)),
            dma,
            dma,
            dma,
            dma,
            dma,
            dma((half,)),
            dma,
            dma((half,)),
            dma,
            dma,
        ],
        compiler_params=pltpu.CompilerParams(
            collective_id=0,
            has_side_effects=True,
            vmem_limit_bytes=62 * 1024 * 1024,
        ),
        name="layer",
    )(*operands)


def solution(mesh):
    return jax.shard_map(
        body,
        mesh=mesh,
        in_specs=(
            P(("grp", "sp"), "tp"),
            P(("grp", "sp"), None),
            P(("grp", "sp"), None),
            P(),
            P(),
            P(("grp", "sp", "tp"), None),
            P("tp", None),
            P(),
            P(),
            P("sp", "tp"),
            P("sp", "tp"),
            P(None, "tp"),
            P(None, "tp"),
            P("sp", "tp"),
        ),
        out_specs=P(("grp", "sp", "tp"), None),
        check_vma=False,
    )
```
